32 devices in a mesh: ep: 4 (over y, x), tp: 8 (over z, core).
Axes of the slice: x: 2, y: 2, z: 4, core: 2. Of those that a mesh axis runs over, the one named last changes fastest.
Arguments:
- pool_in: bfloat16 [16384, 1024], P(('ep', 'tp')), may hold values from -6 to 6
- pool_weight: bfloat16 [4, 256, 256], replicated, may hold values from -0.375 to 0.375
- pool_gain: float32 [1024], replicated, may hold values from 0.1 to 1.9
- out_weight: bfloat16 [1024, 2048], P('tp'), may hold values from -0.1875 to 0.1875
- mix_gain: float32 [2048], replicated, may hold values from 0.1 to 1.9
- expert_in: bfloat16 [1024, 2048], P('ep'), may hold values from -6 to 6
- routes: int32 [1024, 4], P('ep'), may hold values from 0 to 7, all different within a row; in each aligned block of 32 rows (0 to 31, 32 to 63, ...) at most 32 rows name the same one
- route_weight: float32 [1024, 4], P('ep'), may hold values from 0.1 to 1
- pre_gain: float32 [2048], replicated, may hold values from 0.1 to 1.9
- gate_weight: bfloat16 [8, 2048, 4096], P('ep', None, 'tp'), may hold values from -0.39648438 to 0.39648438
- up_weight: bfloat16 [8, 2048, 4096], P('ep', None, 'tp'), may hold values from -0.39648438 to 0.39648438
- down_weight: bfloat16 [8, 4096, 2048], P('ep', 'tp'), may hold values from -0.09375 to 0.09375
- post_gain: float32 [2048], replicated, may hold values from 0.1 to 1.9
Outputs:
- mix_out: bfloat16 [16384, 2048], P(('ep', 'tp'))
- expert_out: bfloat16 [1024, 2048], P(('ep', 'tp'))
The draws below stay inside these ranges and needn't reach their ends.
Inputs may be any that keep to these rules, and one draw needn't show every extreme that they name: `routes`: each row names 4 different experts. In each aligned block of 32 rows no expert is named by more than 32 rows, a bound that some block reaches.
All inputs are finite; a program needn't handle non-finite values.
Results may differ from the reference program's by a relative error of at most 0.019.
Values may be sent and summed in bfloat16 or wider, within the bound.
A program may use at most 128 MiB of HBM per device.

```python
import math
import jax
import jax.numpy as jnp
import numpy as np
from jax import lax

D = 2048
DP = 1024
GROUP = 256
FF = 4096
EXPERTS = 8
TOPK = 4
MOE_TOK = 1024
MIX_TOK = 16384
SUB = 32
CAP = 32
N_TP = 8


def shard_levels(rng, dims, cuts, least, high):
    level, own = 1.0, jax.random.fold_in(rng, 6)
    for dim, shards_of in cuts:
        heights = jnp.exp(jax.random.uniform(jax.random.fold_in(own, dim), (shards_of,), jnp.float32, least / len(cuts), high / len(cuts)))
        level = level * jnp.repeat(heights, dims[dim] // shards_of).reshape([-1 if axis == dim else 1 for axis in range(len(dims))])
    return level


def deal_out(rng, own, number, rows, count, top, most, lean):
    order = jax.random.permutation(rng, count)
    heavy_load, common = portions_of(count, rows * top, most, lean, True), portions_of(count, rows * top, most, lean, False)
    places = jnp.arange(count)

    def named(sizes, turn):
        used = int((sizes > 0).sum())
        fixed = max(1, used // 4)
        passed = fixed + (places - fixed + turn * (used - fixed)) % max(1, count - fixed)
        return jnp.zeros((count,), jnp.int32).at[order[jnp.where(places < fixed, places, passed)]].set(jnp.asarray(sizes, jnp.int32))

    sizes = jnp.where(number % 4 == 0, named(heavy_load, number // 4), named(common, number - number // 4 - 1))
    mixed = jax.random.permutation(jax.random.fold_in(own, 3), count)
    giver, sink = mixed[0:count // 2 * 2:2], mixed[1:count // 2 * 2:2]
    margin = jnp.minimum(sizes[giver] - 1, most - sizes[sink]) // 2
    margin = jnp.where((giver == order[0]) | (sink == order[0]) | (sizes[sink] == 0), 0, jnp.maximum(margin, 0))
    passed = jax.random.randint(jax.random.fold_in(own, 4), (count // 2,), 0, 1 << 20) % (margin + 1)
    sizes = sizes.at[giver].add(-passed).at[sink].add(passed)
    labels = jnp.searchsorted(jnp.cumsum(sizes), jnp.arange(rows * top), side="right").astype(jnp.int32)
    listing = labels.reshape(top, rows).T
    listing = listing[jax.random.permutation(jax.random.fold_in(own, 1), rows)]
    turn = jax.random.randint(jax.random.fold_in(own, 2), (rows, 1), 0, top)
    return jnp.take_along_axis(listing, (jnp.arange(top)[None, :] + turn) % top, axis=1)


def portions_of(count, total, limit, lean, full):
    portions = [(1 << 20) // math.isqrt(standing ** lean) + 1 for standing in range(1, count + 1)]
    largest = limit if full else min(limit, max(-(-total // count), total * portions[0] // sum(portions)))
    least = 1 if total - largest >= count - 1 else 0
    given, surplus = [largest] + [least] * (count - 1), total - largest - least * (count - 1)
    while surplus > 0:
        candidates = [i for i in range(1, count) if given[i] < largest] or [i for i in range(1, count) if given[i] < limit]
        pool, left = sum([portions[i] for i in candidates]), surplus
        for i in candidates:
            more = min(limit - given[i], max(1, left * portions[i] // pool), surplus)
            given[i] = given[i] + more
            surplus = surplus - more
    return np.array(given)


def noise(rng, extent, width, most, cuts=(), held_as=jnp.bfloat16):
    level = shard_levels(rng, extent, cuts, -0.22, 0.18) if cuts else 1.0
    array = jax.random.normal(rng, extent, jnp.float32) * width * level
    return jnp.minimum(jnp.maximum(array, -most), most).astype(held_as)


def setup_inputs(seed: int = 0) -> dict:
    splits = jax.random.split(jax.random.key(seed), 14)
    pool_in = noise(splits[0], (MIX_TOK, DP), 1.0, 6.0, ((0, 32),))
    pool_weight = noise(splits[1], (4, GROUP, GROUP), GROUP ** -0.5, 0.375)
    pool_gain = jnp.clip(1.0 + 0.18 * jax.random.normal(splits[2], (DP,), jnp.float32), 0.1, 1.9)
    out_weight = noise(splits[3], (DP, D), DP ** -0.5, 0.1875, ((0, 8),))
    mix_gain = jnp.clip(1.0 + 0.18 * jax.random.normal(splits[4], (D,), jnp.float32), 0.1, 1.9)
    expert_in = noise(splits[5], (MOE_TOK, D), 1.0, 6.0, ((0, 4),))
    routes_keys = jax.random.split(jax.random.fold_in(splits[6], 1), MOE_TOK // SUB)
    routes_turns = jax.random.permutation(jax.random.fold_in(splits[6], 3), MOE_TOK // SUB)
    routes = jax.vmap(lambda own, number: deal_out(jax.random.fold_in(splits[6], 2), own, number, SUB, EXPERTS, TOPK, CAP, 2))(routes_keys, routes_turns).reshape((MOE_TOK, TOPK))
    route_weight = jnp.clip(jnp.exp(math.log(1.0) - 2.3025851 * jax.random.uniform(splits[7], (MOE_TOK, TOPK), jnp.float32) ** shard_levels(splits[7], (MOE_TOK, TOPK), ((0, 4),), -0.2, 0.2)), 0.1, 1.0)
    pre_gain = jnp.clip(1.0 + 0.18 * jax.random.normal(splits[8], (D,), jnp.float32), 0.1, 1.9)
    gate_weight = noise(splits[9], (EXPERTS, D, FF), (3.0 * D ** -0.5), 0.39648438, ((0, 4), (2, 8)))
    up_weight = noise(splits[10], (EXPERTS, D, FF), (3.0 * D ** -0.5), 0.39648438, ((0, 4), (2, 8)))
    down_weight = noise(splits[11], (EXPERTS, FF, D), FF ** -0.5, 0.09375, ((0, 4), (1, 8)))
    post_gain = jnp.clip(1.0 + 0.18 * jax.random.normal(splits[12], (D,), jnp.float32), 0.1, 1.9)
    return {"pool_in": pool_in, "pool_weight": pool_weight, "pool_gain": pool_gain, "out_weight": out_weight, "mix_gain": mix_gain, "expert_in": expert_in, "routes": routes, "route_weight": route_weight, "pre_gain": pre_gain, "gate_weight": gate_weight, "up_weight": up_weight, "down_weight": down_weight, "post_gain": post_gain}


WINDOWS = (2, 4, 8, 16)
EPS = 1e-06
LIMIT = 7.0
ALPHA = 1.702

def rms_scale(values, gain):
    mean_square = lax.optimization_barrier(jnp.mean(values * values, axis=-1, keepdims=True))
    return values * lax.rsqrt(mean_square + EPS) * gain.astype(jnp.float32)

def trailing_pool(padded, first_pos, rows):
    group = padded.shape[1] // 4
    position = first_pos + jnp.arange(rows, dtype=jnp.int32)
    pieces = []
    for which, window in enumerate(WINDOWS):
        channels = padded[:, which * group:(which + 1) * group]
        running = channels[16:16 + rows]
        for reach in range(2, window + 1):
            running = running + channels[17 - reach:17 - reach + rows]
        count = jnp.minimum(position + 1, window).astype(jnp.float32)[:, None]
        pieces.append(running / count)
    pooled = jnp.concatenate(pieces, axis=1)
    return (pooled - padded[16:]).astype(jnp.bfloat16)

def selection(block_routes, experts, capacity):
    flat = block_routes.reshape(-1)
    onehot = (flat[:, None] == jnp.arange(experts, dtype=jnp.int32)[None, :]).astype(jnp.int32)
    earlier = jnp.cumsum(onehot, axis=0) - onehot
    rank = lax.optimization_barrier(jnp.sum(earlier * onehot, axis=1))
    slots = (flat * capacity + rank).reshape(block_routes.shape)
    return (slots[:, :, None] == jnp.arange(experts * capacity, dtype=jnp.int32)[None, None, :]).astype(jnp.bfloat16)

def clamped_unit(gate, up):
    gate = jnp.minimum(gate, LIMIT)
    up = jnp.clip(up, -LIMIT, LIMIT)
    return (up + 1.0) * gate * jax.nn.sigmoid(ALPHA * gate)

def expert_rows(rows, gate_w, up_w, down_w):
    gate = jnp.dot(rows, gate_w, preferred_element_type=jnp.float32)
    up = jnp.dot(rows, up_w, preferred_element_type=jnp.float32)
    hidden = clamped_unit(gate, up).astype(jnp.bfloat16)
    parts = hidden.reshape(rows.shape[0], N_TP, FF // N_TP).astype(jnp.float32)
    slices = down_w.reshape(N_TP, FF // N_TP, D).astype(jnp.float32)
    partial_value = jnp.einsum('rtf,tfd->rtd', parts, slices).astype(jnp.bfloat16)
    partial_value = lax.optimization_barrier(partial_value)
    return lax.optimization_barrier(jnp.sum(partial_value.astype(jnp.float32), axis=1)).astype(jnp.bfloat16)

def reference(pool_in, pool_weight, pool_gain, out_weight, mix_gain, expert_in, routes, route_weight, pre_gain, gate_weight, up_weight, down_weight, post_gain):
    rows = pool_in.shape[0]
    padded = jnp.concatenate([jnp.zeros((16, pool_in.shape[1]), jnp.float32), pool_in.astype(jnp.float32)], axis=0)
    diff = trailing_pool(padded, jnp.int32(0), rows)
    grouped = diff.reshape(rows, 4, GROUP).astype(jnp.float32)
    mixed = jnp.einsum('sgc,gcd->sgd', grouped, pool_weight.astype(jnp.float32))
    mixed = (mixed.reshape(rows, DP) * pool_gain.astype(jnp.float32)).astype(jnp.bfloat16)
    projected = jnp.dot(mixed, out_weight, preferred_element_type=jnp.float32)
    mix_out = rms_scale(projected, mix_gain).astype(jnp.bfloat16)
    normed = rms_scale(expert_in.astype(jnp.float32), pre_gain).astype(jnp.bfloat16)
    blocks = routes.shape[0] // SUB
    picks = jax.vmap(lambda block: selection(block, EXPERTS, CAP))(routes.reshape(blocks, SUB, TOPK)).astype(jnp.float32)
    token_picks = lax.optimization_barrier(jnp.sum(picks, axis=2))
    buffers = jnp.einsum('bts,btd->bsd', token_picks, normed.reshape(blocks, SUB, D).astype(jnp.float32)).astype(jnp.bfloat16)
    gathered = buffers.reshape(blocks, EXPERTS, CAP, D).transpose(1, 0, 2, 3).reshape(EXPERTS, blocks * CAP, D)
    outputs = lax.map(lambda operands: expert_rows(*operands), (gathered, gate_weight, up_weight, down_weight))
    back = outputs.reshape(EXPERTS, blocks, CAP, D).transpose(1, 0, 2, 3).reshape(blocks, EXPERTS * CAP, D).astype(jnp.float32)
    per_route = jnp.einsum('btks,bsd->btkd', picks, back)
    weights = route_weight.reshape(blocks, SUB, TOPK).astype(jnp.float32)
    combined = lax.optimization_barrier(jnp.sum(per_route * weights[..., None], axis=2)).reshape(blocks * SUB, D)
    expert_out = rms_scale(combined, post_gain).astype(jnp.bfloat16)
    return (mix_out, expert_out)
```

```python
import functools
import math

import jax
import jax.numpy as jnp
from jax import lax
from jax.experimental import pallas as pl
from jax.experimental.pallas import tpu as pltpu
from jax.sharding import PartitionSpec as P

WINDOWS = (2, 4, 8, 16)
EPS = 1e-06
LIMIT = 7.0
ALPHA = 1.702
TILE = 256
WIDE = 512
LAG = 2
POOL_ROWS = 128
PROJECT_ROWS = 256
SUBS = 2
MESH = pl.DeviceIdType.MESH


def rms_scale(values, gain):
    mean_square = jnp.mean(values * values, axis=-1, keepdims=True)
    return values * lax.rsqrt(mean_square + EPS) * gain


def clamped_unit(gate, up):
    gate = jnp.minimum(gate, LIMIT)
    up = jnp.clip(up, -LIMIT, LIMIT)
    return (up + 1.0) * gate * jax.nn.sigmoid(ALPHA * gate)


def flipped(place, mask, count):
    result, bit = 0, 1
    while bit < count:
        result = result + ((place // bit + mask // bit) % 2) * bit
        bit *= 2
    return result


def each(count, step):
    if count == 1:
        step(0)
    else:
        pl.loop(0, count)(step)


def both(first, second):
    return jnp.logical_and(first, second)


def mixer_kernel(
    n_ep,
    n_tp,
    expert_hbm,
    routes_ref,
    route_weight_ref,
    pre_gain_ref,
    gate_hbm,
    up_hbm,
    down_hbm,
    gain_ref,
    pool_hbm,
    pool_weight_hbm,
    pool_gain_ref,
    out_weight_hbm,
    mix_gain_ref,
    mix_ref,
    out_ref,
    in_ref,
    own_ref,
    padded_ref,
    mixed_ref,
    pool_weight_ref,
    all_weight_ref,
    own_table_ref,
    table_ref,
    x_ref,
    gate_ref,
    up_ref,
    down_ref,
    hid_ref,
    part_ref,
    core_ref,
    first_ref,
    second_ref,
    acc_ref,
    zsend_ref,
    zrecv_ref,
    load_sem,
    table_send,
    table_recv,
    ag_send,
    ag_recv,
    pair_send,
    pair_recv,
    cs_send,
    cs_recv,
    first_send,
    first_recv,
    second_send,
    second_recv,
    z_send,
    z_recv,
    rim_send,
    rim_recv,
    w_send,
    w_recv,
    wp_send,
    wp_recv,
):
    ep, tp = lax.axis_index("ep"), lax.axis_index("tp")
    core, z = tp % 2, tp // 2
    partner = z * 2 + 1 - core
    n_z = n_tp // 2
    side = math.isqrt(n_ep)
    others = side - 1
    y, x = ep // side, ep % side
    tokens, width = in_ref.shape
    experts = gate_ref.shape[0]
    tiles = width // TILE
    half_tiles = tiles // 2
    half_z = n_z // 2
    piece = tokens // 2
    share = piece // 2
    own = n_ep - 1
    rows = padded_ref.shape[0] - POOL_ROWS
    channels = padded_ref.shape[1]
    sub_rows = out_weight_hbm.shape[0] // SUBS

    def remote(source, target, send, recv, device):
        return pltpu.make_async_remote_copy(
            source, target, send, recv, device_id=device, device_id_type=MESH
        )

    def x_peer(f):
        return {"ep": y * side + flipped(x, f + 1, side)}

    def y_peer(f):
        return {"ep": flipped(y, f + 1, side) * side + x}

    def ep_peer(k):
        return {"ep": flipped(ep, k + 1, n_ep)}

    def z_peer(k):
        return flipped(z, k + 1, n_z)

    place = ep * n_tp + tp
    devices = n_ep * n_tp
    after, before = (place + 1) % devices, (place + devices - 1) % devices

    def at(device):
        return {"ep": device // n_tp, "tp": device % n_tp}

    in_load = pltpu.make_async_copy(expert_hbm, in_ref, load_sem.at[0])
    weight_load = pltpu.make_async_copy(out_weight_hbm, all_weight_ref.at[tp], load_sem.at[1])
    pool_load = pltpu.make_async_copy(
        pool_hbm, padded_ref.at[pl.ds(POOL_ROWS, rows)], load_sem.at[2]
    )
    map_load = pltpu.make_async_copy(pool_weight_hbm, pool_weight_ref, load_sem.at[3])

    def expert_load(e, k):
        source, target = ((gate_hbm, gate_ref), (up_hbm, up_ref), (down_hbm, down_ref))[k]
        return pltpu.make_async_copy(source.at[e], target.at[e], load_sem.at[4 + 3 * e + k])

    for load in (in_load, weight_load, pool_load):
        load.start()
    for e in range(experts):
        for k in range(2):
            expert_load(e, k).start()
    for e in range(experts):
        expert_load(e, 2).start()
    map_load.start()

    barrier = pltpu.get_barrier_semaphore()
    pl.semaphore_signal(barrier, inc=1, device_id=at(after), device_id_type=MESH)
    pl.semaphore_signal(barrier, inc=1, device_id=at(before), device_id_type=MESH)
    pl.semaphore_signal(barrier, inc=1, device_id={"tp": partner}, device_id_type=MESH)
    for k in range(n_ep - 1):
        pl.semaphore_signal(barrier, inc=1, device_id=ep_peer(k), device_id_type=MESH)
    for k in range(n_z - 1):
        pl.semaphore_signal(
            barrier, inc=1, device_id={"tp": z_peer(k) * 2 + core}, device_id_type=MESH
        )

    padded_ref[: POOL_ROWS - 16] = jnp.zeros((POOL_ROWS - 16, channels), jnp.bfloat16)
    lanes = lax.broadcasted_iota(jnp.int32, own_table_ref.shape, 0)
    table = jnp.zeros(own_table_ref.shape, jnp.float32)
    for k in range(routes_ref.shape[0]):
        table = table + jnp.where(
            lanes == routes_ref[k : k + 1, :], route_weight_ref[k : k + 1, :], 0.0
        )
    own_table_ref[...] = table
    in_load.wait()
    own_ref[...] = rms_scale(in_ref[...].astype(jnp.float32), pre_gain_ref[...]).astype(
        jnp.bfloat16
    )
    pl.semaphore_wait(barrier, n_ep + n_z + 1)

    def slot_a(f):
        return f

    def slot_b(f):
        return others + f

    def slot_d(g, f):
        return 2 * others + g * others + f

    def part_rows(p):
        return pl.ds(pl.multiple_of(p * piece + core * share, share), share)

    def gather_copy(source, slot, p, device, sub=None):
        start, size = p * piece + core * share, share
        if sub is not None:
            size = (share // 4, share - share // 4)[sub]
            start = start + sub * (share // 4)
        here = pl.ds(pl.multiple_of(start, share // 4), size)
        k = 0 if sub is None else sub
        return remote(
            source.at[here],
            x_ref.at[slot, here],
            ag_send.at[slot, p, k],
            ag_recv.at[slot, p, k],
            device,
        )

    def early_x(f):
        return gather_copy(own_ref, slot_a(f), 0, x_peer(f))

    def early_y(f):
        return gather_copy(own_ref, slot_a(f), 1, y_peer(f))

    def late_x(f, sub):
        return gather_copy(own_ref, slot_b(f), 1, x_peer(f), sub)

    def late_y(f, sub):
        return gather_copy(own_ref, slot_b(f), 0, y_peer(f), sub)

    def pass_y(g, f):
        return gather_copy(x_ref.at[slot_a(f)], slot_d(g, f), 0, y_peer(g))

    def pass_x(g, f):
        return gather_copy(x_ref.at[slot_a(g)], slot_d(g, f), 1, x_peer(f))

    def pair_copy(slot, p):
        here = part_rows(p)
        return remote(
            x_ref.at[slot, here],
            x_ref.at[slot, here],
            pair_send.at[slot, p],
            pair_recv.at[slot, p],
            {"tp": partner},
        )

    def table_copy(k):
        return remote(
            own_table_ref, table_ref.at[k], table_send.at[k], table_recv.at[k], ep_peer(k)
        )

    def core_copy(slot, j):
        return remote(
            part_ref.at[j, :, 1 - core],
            core_ref.at[slot, j],
            cs_send.at[j],
            cs_recv.at[slot, j],
            {"tp": partner},
        )

    def z_rows(p):
        return pl.ds(p * half_z, half_z)

    def first_copy(h, f, g, jj, p, slot):
        return remote(
            core_ref.at[slot, h * half_tiles + jj, z_rows(p)],
            first_ref.at[h, f, g, jj, p],
            first_send.at[h, f, g, jj, p],
            first_recv.at[h, f, g, jj, p],
            x_peer(f) if h == 0 else y_peer(f),
        )

    def second_slot(h, g, p):
        return slot_a(g) if h != p else slot_b(g)

    def second_copy(h, g, jj, p):
        return remote(
            core_ref.at[second_slot(h, g, p), h * half_tiles + jj, z_rows(p)],
            second_ref.at[h, g, jj, p],
            second_send.at[h, g, jj, p],
            second_recv.at[h, g, jj, p],
            y_peer(g) if h == 0 else x_peer(g),
        )

    levels = n_z.bit_length() - 1

    def z_part(level):
        count = n_z >> (level + 1)
        return (z // (1 << level)) % 2, n_z - 2 * count, count

    def z_copy(level, j):
        _, first, count = z_part(level)
        return remote(
            zsend_ref.at[j, pl.ds(first, count)],
            zrecv_ref.at[j, pl.ds(first, count)],
            z_send.at[level, j],
            z_recv.at[level, j],
            {"tp": flipped(z, 1 << level, n_z) * 2 + core},
        )

    rim_copy = remote(
        padded_ref.at[pl.ds(POOL_ROWS + rows - 16, 16)],
        padded_ref.at[pl.ds(POOL_ROWS - 16, 16)],
        rim_send,
        rim_recv,
        at(after),
    )

    def weight_rows(block, sub):
        return all_weight_ref.at[block, pl.ds(sub * sub_rows, sub_rows)]

    def toward(d, s):
        return z - s if d == 0 else z + s

    def sends(d, s):
        if d == 0:
            return both(z + 1 < n_z, z - s >= 0)
        return both(z >= 1, z + s < n_z)

    def receives(d, s):
        return z - 1 - s >= 0 if d == 0 else z + 1 + s < n_z

    def weight_copy(d, s, sub):
        block = weight_rows(toward(d, s) * 2 + core, sub)
        target = z + 1 if d == 0 else z - 1
        return remote(
            block, block, w_send.at[d, s, sub], w_recv.at[d, s, sub], {"tp": target * 2 + core}
        )

    def weight_arrival(d, s, sub):
        block = weight_rows(toward(d, s + 1) * 2 + core, sub)
        return remote(
            block, block, w_send.at[d, s, sub], w_recv.at[d, s, sub], {"tp": partner}
        )

    def weight_pair(d, s, sub):
        block = weight_rows(toward(d, s + 1) * 2 + core, sub)
        k = 1 + d * (n_z - 1) + s
        return remote(block, block, wp_send.at[k, sub], wp_recv.at[k, sub], {"tp": partner})

    def own_pair(sub):
        block = weight_rows(tp, sub)
        return remote(block, block, wp_send.at[0, sub], wp_recv.at[0, sub], {"tp": partner})

    def weight_step(s, sub):
        for d in range(2):

            @pl.when(receives(d, s))
            def _():
                weight_arrival(d, s, sub).wait_recv()
                weight_pair(d, s, sub).start()

            if s + 1 < n_z - 1:

                @pl.when(sends(d, s + 1))
                def _():
                    weight_copy(d, s + 1, sub).start()

    for f in range(others):
        early_x(f).start()
        early_y(f).start()
    for k in range(n_ep - 1):
        table_copy(k).start()
    for f in range(others):
        late_x(f, 0).start()
        late_y(f, 0).start()
    pool_load.wait()
    rim_copy.start()
    weight_load.wait()
    for sub in range(SUBS):
        for d in range(2):

            @pl.when(sends(d, 0))
            def _():
                weight_copy(d, 0, sub).start()

        own_pair(sub).start()

    def pool():
        rim_copy.wait_recv()

        @pl.when(place == 0)
        def _():
            padded_ref[POOL_ROWS - 16 : POOL_ROWS] = jnp.zeros((16, channels), jnp.bfloat16)

        map_load.wait()
        group = channels // 4
        reach = (
            lax.broadcasted_iota(jnp.int32, (POOL_ROWS, 2 * POOL_ROWS), 0)
            + POOL_ROWS
            - lax.broadcasted_iota(jnp.int32, (POOL_ROWS, 2 * POOL_ROWS), 1)
        )
        local = lax.broadcasted_iota(jnp.int32, (POOL_ROWS, 1), 0)

        @pl.loop(0, rows // POOL_ROWS)
        def _(i):
            start = pl.multiple_of(i * POOL_ROWS, POOL_ROWS)
            here = pl.ds(start, POOL_ROWS)
            there = pl.ds(start + POOL_ROWS, POOL_ROWS)
            position = place * rows + start + local
            for which, window in enumerate(WINDOWS):
                columns = slice(which * group, (which + 1) * group)
                band = jnp.where((reach >= 0) & (reach < window), 1.0, 0.0).astype(jnp.bfloat16)
                running = jnp.dot(
                    band,
                    padded_ref[pl.ds(start, 2 * POOL_ROWS), columns],
                    preferred_element_type=jnp.float32,
                )
                count = jnp.minimum(position + 1, window).astype(jnp.float32)
                diff = running / count - padded_ref[there, columns].astype(jnp.float32)
                mixed = jnp.dot(
                    diff.astype(jnp.bfloat16),
                    pool_weight_ref[which],
                    preferred_element_type=jnp.float32,
                )
                mixed_ref[here, columns] = (mixed * pool_gain_ref[:, columns]).astype(jnp.bfloat16)

    def project(i):
        here = pl.ds(pl.multiple_of(i * PROJECT_ROWS, PROJECT_ROWS), PROJECT_ROWS)
        projected = jnp.dot(
            mixed_ref[here],
            all_weight_ref[...].reshape(channels, width),
            preferred_element_type=jnp.float32,
        )
        mix_ref[here] = rms_scale(projected, mix_gain_ref[...]).astype(jnp.bfloat16)

    def hidden(values_ref, table, first=False):
        lane = lax.broadcasted_iota(jnp.int32, (tokens, table.shape[0]), 1)
        weights = jnp.transpose(table)
        for which in range(experts):
            if first:
                for k in range(2):
                    expert_load(which, k).wait()
            weight = jnp.sum(
                jnp.where(lane == ep * experts + which, weights, 0.0), axis=1, keepdims=True
            )
            values = values_ref[...]
            gate = jnp.dot(values, gate_ref[which], preferred_element_type=jnp.float32)
            up = jnp.dot(values, up_ref[which], preferred_element_type=jnp.float32)
            hid_ref[which] = (clamped_unit(gate, up) * weight).astype(jnp.bfloat16)

    def partial(slot, after, lag=LAG, hook=None):
        def ended(j):
            for k in range(WIDE // TILE):
                core_copy(slot, j + k).wait()
                after((j + k) // half_tiles, (j + k) % half_tiles)

        starts = [
            h * half_tiles + jj for jj in range(0, half_tiles, WIDE // TILE) for h in range(2)
        ]
        for i, j in enumerate(starts):
            columns = slice(j * TILE, j * TILE + WIDE)
            total = jnp.dot(
                hid_ref[0], down_ref[0, :, columns], preferred_element_type=jnp.float32
            )
            for which in range(1, experts):
                total = total + jnp.dot(
                    hid_ref[which], down_ref[which, :, columns], preferred_element_type=jnp.float32
                )
            total = total.astype(jnp.bfloat16)
            for k in range(WIDE // TILE):
                part_ref[j + k] = total[:, k * TILE : (k + 1) * TILE].reshape(part_ref.shape[1:])
                core_copy(slot, j + k).start()
            if i >= lag:
                ended(starts[i - lag])
        if hook is not None:
            hook()
        for j in starts[len(starts) - lag :]:
            ended(j)

    def joined(k0, k1):
        return jnp.concatenate(
            [table_ref[k0, :, :piece], table_ref[k1, :, piece:]], axis=1
        )

    def core_sum(slot, h, jj):
        j = h * half_tiles + jj
        return part_ref[j, :, core].astype(jnp.float32) + core_ref[slot, j].astype(jnp.float32)

    hidden(own_ref, own_table_ref[...], first=True)
    pool()
    for e in range(experts):
        expert_load(e, 2).wait()

    def own_done(h, jj):
        acc_ref[h * half_tiles + jj] = core_sum(own, h, jj)

    steps = [(s, sub) for s in range(n_z - 1) for sub in range(SUBS)]
    last = width // WIDE

    def early_arrived():
        for f in range(others):
            early_x(f).wait_recv()
            early_y(f).wait_recv()
            for g in range(others):
                pass_y(g, f).start()
                pass_x(f, g).start()
            for p in range(2):
                pair_copy(slot_a(f), p).start()
        for f in range(others):
            late_x(f, 1).start()
            late_y(f, 1).start()
        weight_step(*steps[0])

    partial(own, own_done, last, early_arrived)
    for k in range(n_ep - 1):
        table_copy(k).wait_recv()

    def halves():
        return [(h, jj) for jj in range(half_tiles) for h in range(2)]

    def late_pairs():
        for f in range(others):
            for sub in range(2):
                late_x(f, sub).wait_recv()
                late_y(f, sub).wait_recv()
            for p in range(2):
                pair_copy(slot_b(f), p).start()

    def diagonal_pairs():
        for g in range(others):
            for f in range(others):
                pass_y(g, f).wait_recv()
                pass_x(g, f).wait_recv()
                for p in range(2):
                    pair_copy(slot_d(g, f), p).start()

    def batch(slot, k0, k1, send, lag=LAG, hook=None):
        for p in range(2):
            pair_copy(slot, p).wait_recv()
        hidden(x_ref.at[slot], joined(k0, k1))

        def done(h, jj):
            core_ref[slot, h * half_tiles + jj] = core_sum(slot, h, jj).astype(jnp.bfloat16)
            send(h, jj)

        partial(slot, done, lag, hook if others == 1 else None)

    def batch_a(f):
        def send(h, jj):
            first_copy(h, f, 0, jj, h, slot_a(f)).start()

        batch(slot_a(f), f, (f + 1) * side - 1, send, last, diagonal_pairs)

    def batch_d(i):
        g, f = (i // others, i % others) if others > 1 else (0, 0)

        def send(h, jj):
            for p in range(2):
                if h == 0:
                    first_copy(0, f, g + 1, jj, p, slot_d(g, f)).start()
                else:
                    first_copy(1, g, f + 1, jj, p, slot_d(g, f)).start()

        k = (g + 1) * side + f
        batch(slot_d(g, f), k, k, send, LAG, late_pairs)

    def batch_b(f):
        def send(h, jj):
            first_copy(h, f, 0, jj, 1 - h, slot_b(f)).start()

        batch(slot_b(f), (f + 1) * side - 1, f, send)

    each(others, batch_a)
    if others > 1:
        diagonal_pairs()
    weight_step(*steps[1])
    each(others * others, batch_d)
    if others > 1:
        late_pairs()
    weight_step(*steps[2])
    each(others, batch_b)
    weight_step(*steps[3])

    def second_stage(g):
        for late, (h, jj) in [(late, tile) for late in range(2) for tile in halves()]:
            for p in (h if late else 1 - h,):
                slot, j = second_slot(h, g, p), h * half_tiles + jj
                total = core_ref[slot, j, z_rows(p)].astype(jnp.float32)
                for f in range(others):
                    first_copy(h, f, g + 1, jj, p, slot).wait_recv()
                    total = total + first_ref[h, f, g + 1, jj, p].astype(jnp.float32)
                core_ref[slot, j, z_rows(p)] = total.astype(jnp.bfloat16)
                second_copy(h, g, jj, p).start()

    each(others, second_stage)

    def plane_sum(j, h, jj):
        for p in range(2):
            total = acc_ref[j, z_rows(p)]
            for f in range(others):
                first_copy(h, f, 0, jj, p, own).wait_recv()
                total = total + first_ref[h, f, 0, jj, p].astype(jnp.float32)
            for g in range(others):
                second_copy(h, g, jj, p).wait_recv()
                total = total + second_ref[h, g, jj, p].astype(jnp.float32)
            acc_ref[j, z_rows(p)] = total

    def z_level(level, jj):
        for h in range(2):
            j = h * half_tiles + jj
            if level == 0:
                plane_sum(j, h, jj)
            else:
                z_fold(level - 1, j)
            if level < levels:
                bit, first, count = z_part(level)
                for m in range(count):
                    zsend_ref[j, first + m] = acc_ref[j, 2 * m + 1 - bit].astype(jnp.bfloat16)
                z_copy(level, j).start()

    def z_fold(level, j):
        bit, first, count = z_part(level)
        z_copy(level, j).wait_recv()
        for m in range(count):
            acc_ref[j, m] = acc_ref[j, 2 * m + bit] + zrecv_ref[j, first + m].astype(jnp.float32)

    waves = [(level, jj) for level in range(levels) for jj in range(half_tiles)]
    waves.sort(key=lambda wave: (wave[1] + 3 * wave[0], wave[0]))
    rest = steps[4:]
    for wave in waves:
        z_level(*wave)
        if rest:
            weight_step(*rest.pop(0))
    for step in rest:
        weight_step(*step)
    for sub in range(SUBS):
        own_pair(sub).wait_recv()
        for s in range(n_z - 1):
            for d in range(2):

                @pl.when(receives(d, s))
                def _():
                    weight_pair(d, s, sub).wait_recv()

    pl.loop(0, rows // PROJECT_ROWS)(project)

    squares = 0.0
    for jj in range(half_tiles):
        z_level(levels, jj)
        for h in range(2):
            total = acc_ref[h * half_tiles + jj, 0]
            squares = squares + jnp.sum(total * total, axis=-1, keepdims=True)
    scale = lax.rsqrt(squares / width + EPS)
    for j in range(tiles):
        columns = slice(j * TILE, (j + 1) * TILE)
        out_ref[:, columns] = (acc_ref[j, 0] * scale * gain_ref[:, columns]).astype(jnp.bfloat16)

    for f in range(others):
        early_x(f).wait_send()
        early_y(f).wait_send()
        for sub in range(2):
            late_x(f, sub).wait_send()
            late_y(f, sub).wait_send()
        for g in range(others):
            pass_y(g, f).wait_send()
            pass_x(g, f).wait_send()

    @pl.loop(0, n_ep - 1)
    def _(k):
        table_copy(k).wait_send()
        for p in range(2):
            pair_copy(k, p).wait_send()

    for h in range(2):
        for f in range(others):
            for jj in range(half_tiles):
                for p in range(2):
                    for g in range(side):
                        first_copy(h, f, g, jj, p, own).wait_send()
                    second_copy(h, f, jj, p).wait_send()
    for j in range(tiles):
        for level in range(levels):
            z_copy(level, j).wait_send()
    for sub in range(SUBS):
        own_pair(sub).wait_send()
        for s in range(n_z - 1):
            for d in range(2):

                @pl.when(sends(d, s))
                def _():
                    weight_copy(d, s, sub).wait_send()

                @pl.when(receives(d, s))
                def _():
                    weight_pair(d, s, sub).wait_send()

    rim_copy.wait_send()


def fused(operands, n_ep, n_tp):
    expert_in, routes, _, _, gate_weight, up_weight, down_weight = operands[:7]
    pool_in, pool_weight, out_weight = operands[8], operands[9], operands[11]
    tokens, width = expert_in.shape
    rows, channels = pool_in.shape
    experts, _, units = gate_weight.shape
    tiles, n_z, block = width // TILE, n_tp // 2, tokens // n_tp
    side = math.isqrt(n_ep)
    others, half_tiles, half_z = side - 1, tiles // 2, n_z // 2
    dma = pltpu.SemaphoreType.DMA
    vmem = pl.BlockSpec(memory_space=pltpu.VMEM)
    hbm = pl.BlockSpec(memory_space=pltpu.HBM)
    bf16, f32 = jnp.bfloat16, jnp.float32
    buffers = [
        ((tokens, width), bf16),
        ((tokens, width), bf16),
        ((POOL_ROWS + rows, channels), bf16),
        ((rows, channels), bf16),
        (pool_weight.shape, bf16),
        ((n_tp,) + out_weight.shape, bf16),
        ((n_ep * experts, tokens), f32),
        ((n_ep - 1, n_ep * experts, tokens), f32),
        ((n_ep - 1, tokens, width), bf16),
        (gate_weight.shape, bf16),
        (up_weight.shape, bf16),
        (down_weight.shape, bf16),
        ((experts, tokens, units), bf16),
        ((tiles, n_z, 2, block, TILE), bf16),
        ((n_ep, tiles, n_z, block, TILE), bf16),
        ((2, others, side, half_tiles, 2, half_z, block, TILE), bf16),
        ((2, others, half_tiles, 2, half_z, block, TILE), bf16),
        ((tiles, n_z, block, TILE), f32),
        ((tiles, n_z - 1, block, TILE), bf16),
        ((tiles, n_z - 1, block, TILE), bf16),
    ]
    held = sum(math.prod(shape) * jnp.dtype(kind).itemsize for shape, kind in buffers)
    return pl.pallas_call(
        functools.partial(mixer_kernel, n_ep, n_tp),
        out_shape=(pltpu.VMEM((rows, width), bf16), pltpu.VMEM((block, width), bf16)),
        in_specs=[hbm, vmem, vmem, vmem, hbm, hbm, hbm, vmem, hbm, hbm, vmem, hbm, vmem],
        out_specs=(vmem, vmem),
        scratch_shapes=[pltpu.VMEM(shape, kind) for shape, kind in buffers]
        + [
            dma((4 + 3 * experts,)),
            dma((n_ep - 1,)),
            dma((n_ep - 1,)),
            dma((n_ep - 1, 2, 2)),
            dma((n_ep - 1, 2, 2)),
            dma((n_ep - 1, 2)),
            dma((n_ep - 1, 2)),
            dma((tiles,)),
            dma((n_ep, tiles)),
            dma((2, others, side, half_tiles, 2)),
            dma((2, others, side, half_tiles, 2)),
            dma((2, others, half_tiles, 2)),
            dma((2, others, half_tiles, 2)),
            dma((n_z - 1, tiles)),
            dma((n_z - 1, tiles)),
            dma,
            dma,
            dma((2, n_z - 1, SUBS)),
            dma((2, n_z - 1, SUBS)),
            dma((2 * n_z - 1, SUBS)),
            dma((2 * n_z - 1, SUBS)),
        ],
        compiler_params=pltpu.CompilerParams(
            collective_id=0,
            has_side_effects=True,
            vmem_limit_bytes=min(67043328, held + 10 * 2**20),
        ),
        cost_estimate=pl.CostEstimate(
            flops=6 * n_ep * tokens * experts * units * width,
            bytes_accessed=64 * 2**20,
            transcendentals=0,
        ),
        name="mixer_experts",
    )(*(pltpu.with_memory_space_constraint(operand, pltpu.HBM) for operand in operands))


def body(
    pool_in,
    pool_weight,
    pool_gain,
    out_weight,
    mix_gain,
    expert_in,
    routes,
    route_weight,
    pre_gain,
    gate_weight,
    up_weight,
    down_weight,
    post_gain,
):
    n_ep, n_tp = lax.axis_size("ep"), lax.axis_size("tp")
    operands = (
        expert_in,
        routes.T,
        route_weight.T,
        pre_gain[None, :],
        gate_weight,
        up_weight,
        down_weight,
        post_gain[None, :],
        pool_in,
        pool_weight,
        pool_gain[None, :],
        out_weight,
        mix_gain[None, :],
    )
    return fused(operands, n_ep, n_tp)


def solution(mesh):
    return jax.shard_map(
        body,
        mesh=mesh,
        in_specs=(
            P(("ep", "tp"), None),
            P(),
            P(),
            P("tp", None),
            P(),
            P("ep", None),
            P("ep", None),
            P("ep", None),
            P(),
            P("ep", None, "tp"),
            P("ep", None, "tp"),
            P("ep", "tp", None),
            P(),
        ),
        out_specs=(P(("ep", "tp"), None), P(("ep", "tp"), None)),
        check_vma=False,
    )
```

```python
import functools
import math

import jax
import jax.numpy as jnp
from jax import lax
from jax.experimental import pallas as pl
from jax.experimental.pallas import tpu as pltpu
from jax.sharding import PartitionSpec as P

WINDOWS = (2, 4, 8, 16)
EPS = 1e-06
LIMIT = 7.0
ALPHA = 1.702
TILE = 256
WIDE = 512
LAG = 2
POOL_ROWS = 128
PROJECT_ROWS = 256
SUBS = 4
MESH = pl.DeviceIdType.MESH


def rms_scale(values, gain):
    mean_square = jnp.mean(values * values, axis=-1, keepdims=True)
    return values * lax.rsqrt(mean_square + EPS) * gain


def clamped_unit(gate, up):
    gate = jnp.minimum(gate, LIMIT)
    up = jnp.clip(up, -LIMIT, LIMIT)
    return (up + 1.0) * gate * jax.nn.sigmoid(ALPHA * gate)


def flipped(place, mask, count):
    result, bit = 0, 1
    while bit < count:
        result = result + ((place // bit + mask // bit) % 2) * bit
        bit *= 2
    return result


def each(count, step):
    if count == 1:
        step(0)
    else:
        pl.loop(0, count)(step)


def both(first, second):
    return jnp.logical_and(first, second)


def mixer_kernel(
    n_ep,
    n_tp,
    expert_hbm,
    routes_hbm,
    route_weight_hbm,
    pre_gain_hbm,
    gate_hbm,
    up_hbm,
    down_hbm,
    gain_hbm,
    pool_hbm,
    pool_weight_hbm,
    pool_gain_hbm,
    out_weight_hbm,
    mix_gain_hbm,
    mix_ref,
    out_ref,
    routes_ref,
    route_weight_ref,
    pre_gain_ref,
    gain_ref,
    pool_gain_ref,
    mix_gain_ref,
    in_ref,
    own_ref,
    padded_ref,
    mixed_ref,
    pool_weight_ref,
    all_weight_ref,
    own_table_ref,
    table_ref,
    x_ref,
    gate_ref,
    up_ref,
    down_ref,
    hid_ref,
    part_ref,
    core_ref,
    first_ref,
    second_ref,
    acc_ref,
    zsend_ref,
    zrecv_ref,
    ysend_ref,
    yrecv_ref,
    load_sem,
    table_send,
    table_recv,
    ag_send,
    ag_recv,
    pair_send,
    pair_recv,
    cs_send,
    cs_recv,
    first_send,
    first_recv,
    second_send,
    second_recv,
    z_send,
    z_recv,
    y_send,
    y_recv,
    rim_send,
    rim_recv,
    w_send,
    w_recv,
    wp_send,
    wp_recv,
):
    ep, tp = lax.axis_index("ep"), lax.axis_index("tp")
    core, z = tp % 2, tp // 2
    partner = z * 2 + 1 - core
    n_z = n_tp // 2
    side = math.isqrt(n_ep)
    others = side - 1
    y, x = ep // side, ep % side
    tokens, width = in_ref.shape
    experts = gate_ref.shape[0]
    tiles = width // TILE
    half_tiles = tiles // 2
    half_z = n_z // 2
    piece = tokens // 2
    share = piece // 2
    own = n_ep - 1
    pack = WIDE // TILE
    rows = padded_ref.shape[0] - POOL_ROWS
    channels = padded_ref.shape[1]
    sub_rows = out_weight_hbm.shape[0] // SUBS

    def remote(source, target, send, recv, device):
        return pltpu.make_async_remote_copy(
            source, target, send, recv, device_id=device, device_id_type=MESH
        )

    def x_peer(f):
        return {"ep": y * side + flipped(x, f + 1, side)}

    def y_peer(f):
        return {"ep": flipped(y, f + 1, side) * side + x}

    def ep_peer(k):
        return {"ep": flipped(ep, k + 1, n_ep)}

    def z_peer(k):
        return flipped(z, k + 1, n_z)

    place = ep * n_tp + tp
    devices = n_ep * n_tp
    after, before = (place + 1) % devices, (place + devices - 1) % devices

    def at(device):
        return {"ep": device // n_tp, "tp": device % n_tp}

    barrier = pltpu.get_barrier_semaphore()
    pl.semaphore_signal(barrier, inc=1, device_id=at(after), device_id_type=MESH)
    pl.semaphore_signal(barrier, inc=1, device_id=at(before), device_id_type=MESH)
    pl.semaphore_signal(barrier, inc=1, device_id={"tp": partner}, device_id_type=MESH)
    for k in range(n_ep - 1):
        pl.semaphore_signal(barrier, inc=1, device_id=ep_peer(k), device_id_type=MESH)
    for k in range(n_z - 1):
        pl.semaphore_signal(
            barrier, inc=1, device_id={"tp": z_peer(k) * 2 + core}, device_id_type=MESH
        )

    quarters = [
        pl.ds(pl.multiple_of(p * piece + side_of * share, share), share)
        for side_of in (core, 1 - core)
        for p in range(2)
    ]
    pairs = (
        (pre_gain_hbm, pre_gain_ref),
        *((expert_hbm.at[rows_of], in_ref.at[rows_of]) for rows_of in quarters),
        (routes_hbm, routes_ref),
        (route_weight_hbm, route_weight_ref),
        (out_weight_hbm, all_weight_ref.at[tp]),
        (pool_hbm, padded_ref.at[pl.ds(POOL_ROWS, rows)]),
        (pool_weight_hbm, pool_weight_ref),
        (pool_gain_hbm, pool_gain_ref),
        (gain_hbm, gain_ref),
        (mix_gain_hbm, mix_gain_ref),
    )
    loads = [
        pltpu.make_async_copy(source, target, load_sem.at[k])
        for k, (source, target) in enumerate(pairs)
    ]

    def expert_load(e, k):
        source, target = ((gate_hbm, gate_ref), (up_hbm, up_ref), (down_hbm, down_ref))[k]
        return pltpu.make_async_copy(
            source.at[e], target.at[e], load_sem.at[len(pairs) + 3 * e + k]
        )

    for k in (0, 1, 2, 8, 3, 4, 5, 6, 7):
        loads[k].start()
    for e in range(experts):
        for k in range(2):
            expert_load(e, k).start()
    for load in loads[9:]:
        load.start()
    for e in range(experts):
        expert_load(e, 2).start()

    def norm(rows_of):
        own_ref[rows_of] = rms_scale(
            in_ref[rows_of].astype(jnp.float32), pre_gain_ref[...]
        ).astype(jnp.bfloat16)

    loads[0].wait()
    for k in range(2):
        loads[1 + k].wait()
        norm(quarters[k])
    pl.semaphore_wait(barrier, n_ep + n_z + 1)

    def slot_a(f):
        return f

    def slot_d(g, f):
        return others + g * others + f

    def slot_b(f):
        return others + others * others + f

    def turn(slot):
        return (slot + 1) % n_ep % 2

    def part_rows(p):
        return pl.ds(pl.multiple_of(p * piece + core * share, share), share)

    def half_rows(p, sub):
        size = share // 2
        return pl.ds(pl.multiple_of(p * piece + core * share + sub * size, size), size)

    def gather_copy(source, slot, p, sub, device, together=False):
        here = half_rows(p, sub)
        return remote(
            source.at[here],
            x_ref.at[slot, here],
            ag_send,
            ag_recv.at[slot, 0 if together else sub],
            device,
        )

    def gathered(slot, sub, count):
        here = x_ref.at[slot, pl.ds(0, count)]
        return remote(here, here, ag_send, ag_recv.at[slot, sub], {"tp": partner})

    def early_x(f, sub):
        return gather_copy(own_ref, slot_a(f), 0, sub, x_peer(f))

    def early_y(f, sub):
        return gather_copy(own_ref, slot_a(f), 1, sub, y_peer(f))

    def late_x(f, sub):
        return gather_copy(own_ref, slot_b(f), 1, sub, x_peer(f), True)

    def late_y(f, sub):
        return gather_copy(own_ref, slot_b(f), 0, sub, y_peer(f), True)

    def pass_y(g, f, sub):
        return gather_copy(x_ref.at[slot_a(f)], slot_d(g, f), 0, sub, y_peer(g))

    def pass_x(g, f, sub):
        return gather_copy(x_ref.at[slot_a(g)], slot_d(g, f), 1, sub, x_peer(f))

    def pair_copy(slot, p, sub):
        here = half_rows(p, sub)
        return remote(
            x_ref.at[slot, here],
            x_ref.at[slot, here],
            pair_send,
            pair_recv.at[slot],
            {"tp": partner},
        )

    def paired(slot):
        here = x_ref.at[slot, pl.ds(0, piece)]
        return remote(here, here, pair_send, pair_recv.at[slot], {"tp": partner})

    def table_copy(k):
        return remote(
            own_table_ref, table_ref.at[k], table_send, table_recv, ep_peer(k)
        )

    def core_copy(slot, j):
        return remote(
            part_ref.at[pl.ds(j, pack), :, 1 - core],
            core_ref.at[slot, pl.ds(j, pack)],
            cs_send,
            cs_recv.at[turn(slot), j // pack],
            {"tp": partner},
        )

    def core_sent(slot):
        return remote(core_ref.at[slot], core_ref.at[slot], cs_send, rim_recv, {"tp": partner})

    def z_rows(p):
        return pl.ds(p * half_z, half_z)

    def first_copy(h, f, g, jj, p, slot):
        return remote(
            core_ref.at[slot, h * half_tiles + jj, z_rows(p)],
            first_ref.at[h, f, g, jj, z_rows(p)],
            first_send,
            first_recv.at[h, f, g, jj],
            x_peer(f) if h == 0 else y_peer(f),
        )

    def whole_copy(h, f, g, jj, slot):
        return remote(
            core_ref.at[slot, h * half_tiles + jj],
            first_ref.at[h, f, g, jj],
            first_send,
            first_recv.at[h, f, g, jj],
            x_peer(f) if h == 0 else y_peer(f),
        )

    def second_slot(h, g, p):
        return slot_a(g) if h != p else slot_b(g)

    def second_copy(h, g, jj, p):
        return remote(
            core_ref.at[second_slot(h, g, p), h * half_tiles + jj, z_rows(p)],
            second_ref.at[h, g, jj, z_rows(p)],
            second_send,
            second_recv.at[h, g, jj],
            y_peer(g) if h == 0 else x_peer(g),
        )

    def second_arrival(h, g, jj):
        here = second_ref.at[h, g, jj]
        return remote(here, here, second_send, second_recv.at[h, g, jj], {"tp": partner})

    levels = n_z.bit_length() - 1

    def z_part(level):
        count = n_z >> (level + 1)
        return (z // (1 << level)) % 2, n_z - 2 * count, count

    def z_copy(level, j):
        _, first, count = z_part(level)
        return remote(
            zsend_ref.at[j, pl.ds(first, count)],
            zrecv_ref.at[j, pl.ds(first, count)],
            z_send,
            z_recv.at[level, j],
            {"tp": flipped(z, 1 << level, n_z) * 2 + core},
        )

    rim_copy = remote(
        padded_ref.at[pl.ds(POOL_ROWS + rows - 16, 16)],
        padded_ref.at[pl.ds(POOL_ROWS - 16, 16)],
        rim_send,
        rim_recv,
        at(after),
    )

    def weight_rows(block, sub):
        return all_weight_ref.at[block, pl.ds(sub * sub_rows, sub_rows)]

    def toward(d, s):
        return z - s if d == 0 else z + s

    def sends(d, s):
        if d == 0:
            return both(z + 1 < n_z, z - s >= 0)
        return both(z >= 1, z + s < n_z)

    def receives(d, s):
        return z - 1 - s >= 0 if d == 0 else z + 1 + s < n_z

    def weight_copy(d, s, sub):
        block = weight_rows(toward(d, s) * 2 + core, sub)
        target = z + 1 if d == 0 else z - 1
        return remote(
            block, block, w_send, w_recv.at[d, s, sub], {"tp": target * 2 + core}
        )

    def weight_arrival(d, s, sub):
        block = weight_rows(toward(d, s + 1) * 2 + core, sub)
        return remote(
            block, block, w_send, w_recv.at[d, s, sub], {"tp": partner}
        )

    def weight_pair(d, s, sub):
        block = weight_rows(toward(d, s + 1) * 2 + core, sub)
        return remote(block, block, wp_send, wp_recv, {"tp": partner})

    def own_pair(sub):
        block = weight_rows(tp, sub)
        return remote(block, block, wp_send, wp_recv, {"tp": partner})

    def weight_blocks(count):
        here = all_weight_ref.at[pl.ds(0, count)]
        return remote(here, here, w_send, wp_recv, {"tp": partner})

    def weight_pairs():
        here = all_weight_ref.at[pl.ds(0, n_z)]
        return remote(here, here, wp_send, wp_recv, {"tp": partner})

    def weight_step(s, sub):
        for d in range(2):

            @pl.when(receives(d, s))
            def _():
                weight_arrival(d, s, sub).wait_recv()
                weight_pair(d, s, sub).start()

            if s + 1 < n_z - 1:

                @pl.when(sends(d, s + 1))
                def _():
                    weight_copy(d, s + 1, sub).start()

    for sub in range(2):
        for f in range(others):
            early_x(f, sub).start()
            early_y(f, sub).start()
        if sub == 0:
            loads[8].wait()
            rim_copy.start()
    loads[7].wait()
    for sub in range(SUBS):
        for d in range(2):

            @pl.when(sends(d, 0))
            def _():
                weight_copy(d, 0, sub).start()

        own_pair(sub).start()
    for k in (5, 6):
        loads[k].wait()
    lanes = lax.broadcasted_iota(jnp.int32, own_table_ref.shape, 0)
    table = jnp.zeros(own_table_ref.shape, jnp.float32)
    for k in range(routes_ref.shape[0]):
        table = table + jnp.where(
            lanes == routes_ref[k : k + 1, :], route_weight_ref[k : k + 1, :], 0.0
        )
    own_table_ref[...] = table
    for k in range(n_ep - 1):
        table_copy(k).start()
    for k in range(2, 4):
        loads[1 + k].wait()
        norm(quarters[k])
    padded_ref[: POOL_ROWS - 16] = jnp.zeros((POOL_ROWS - 16, channels), jnp.bfloat16)

    def pool():
        rim_copy.wait_recv()

        @pl.when(place == 0)
        def _():
            padded_ref[POOL_ROWS - 16 : POOL_ROWS] = jnp.zeros((16, channels), jnp.bfloat16)

        for k in (9, 10):
            loads[k].wait()
        group = channels // 4
        reach = (
            lax.broadcasted_iota(jnp.int32, (POOL_ROWS, 2 * POOL_ROWS), 0)
            + POOL_ROWS
            - lax.broadcasted_iota(jnp.int32, (POOL_ROWS, 2 * POOL_ROWS), 1)
        )
        local = lax.broadcasted_iota(jnp.int32, (POOL_ROWS, 1), 0)

        @pl.loop(0, rows // POOL_ROWS)
        def _(i):
            start = pl.multiple_of(i * POOL_ROWS, POOL_ROWS)
            here = pl.ds(start, POOL_ROWS)
            there = pl.ds(start + POOL_ROWS, POOL_ROWS)
            position = place * rows + start + local
            for which, window in enumerate(WINDOWS):
                columns = slice(which * group, (which + 1) * group)
                band = jnp.where((reach >= 0) & (reach < window), 1.0, 0.0).astype(jnp.bfloat16)
                running = jnp.dot(
                    band,
                    padded_ref[pl.ds(start, 2 * POOL_ROWS), columns],
                    preferred_element_type=jnp.float32,
                )
                count = jnp.minimum(position + 1, window).astype(jnp.float32)
                diff = running / count - padded_ref[there, columns].astype(jnp.float32)
                mixed = jnp.dot(
                    diff.astype(jnp.bfloat16),
                    pool_weight_ref[which],
                    preferred_element_type=jnp.float32,
                )
                mixed_ref[here, columns] = (mixed * pool_gain_ref[:, columns]).astype(jnp.bfloat16)

    def project(i):
        here = pl.ds(i * PROJECT_ROWS, PROJECT_ROWS)
        projected = jnp.dot(
            mixed_ref[here],
            all_weight_ref[...].reshape(channels, width),
            preferred_element_type=jnp.float32,
        )
        mix_ref[here] = rms_scale(projected, mix_gain_ref[...]).astype(jnp.bfloat16)

    def hidden(values_ref, table, first=False):
        lane = lax.broadcasted_iota(jnp.int32, (tokens, table.shape[0]), 1)
        weights = jnp.transpose(table)
        for which in range(experts):
            if first:
                for k in range(2):
                    expert_load(which, k).wait()
            weight = jnp.sum(
                jnp.where(lane == ep * experts + which, weights, 0.0), axis=1, keepdims=True
            )
            values = values_ref[...]
            gate = jnp.dot(values, gate_ref[which], preferred_element_type=jnp.float32)
            up = jnp.dot(values, up_ref[which], preferred_element_type=jnp.float32)
            hid_ref[which] = (clamped_unit(gate, up) * weight).astype(jnp.bfloat16)

    last = width // WIDE

    def partial(slot, after, lag=LAG, hook=None, at=None):
        def ended(j):
            core_copy(slot, j).wait_recv()
            for k in range(pack):
                after((j + k) // half_tiles, (j + k) % half_tiles)

        starts = [
            h * half_tiles + jj for jj in range(0, half_tiles, pack) for h in range(2)
        ]
        for i, j in enumerate(starts):
            columns = slice(j * TILE, j * TILE + WIDE)
            total = jnp.dot(
                hid_ref[0], down_ref[0, :, columns], preferred_element_type=jnp.float32
            )
            for which in range(1, experts):
                total = total + jnp.dot(
                    hid_ref[which], down_ref[which, :, columns], preferred_element_type=jnp.float32
                )
            total = total.astype(jnp.bfloat16)
            for k in range(pack):
                part_ref[j + k] = total[:, k * TILE : (k + 1) * TILE].reshape(part_ref.shape[1:])
            core_copy(slot, j).start()
            if i >= lag:
                ended(starts[i - lag])
            if hook is not None and i == (last - 1 if at is None else at):
                hook()

        def finish():
            for j in starts[len(starts) - lag :]:
                ended(j)
            core_sent(slot).wait_send()

        return finish

    def joined(k0, k1):
        return jnp.concatenate(
            [table_ref[k0, :, :piece], table_ref[k1, :, piece:]], axis=1
        )

    def core_sum(slot, h, jj):
        j = h * half_tiles + jj
        return part_ref[j, :, core].astype(jnp.float32) + core_ref[slot, j].astype(jnp.float32)

    hidden(own_ref, own_table_ref[...], first=True)
    pool()
    for e in range(experts):
        expert_load(e, 2).wait()

    def own_done(h, jj):
        acc_ref[h * half_tiles + jj] = core_sum(own, h, jj)

    steps = [(s, sub) for s in range(n_z - 1) for sub in range(SUBS)]

    def weight_steps(count):
        for step in steps[:count]:
            weight_step(*step)
        del steps[:count]


    def early_arrived(sub):
        for f in range(others):
            gathered(slot_a(f), sub, share).wait_recv()
            for g in range(others):
                pass_y(g, f, sub).start()
                pass_x(f, g, sub).start()
            for p in range(2):
                pair_copy(slot_a(f), p, sub).start()

    def early_ended():
        early_arrived(1)
        weight_steps(1)

    early_arrived(0)
    partial(own, own_done, last, early_ended)()
    tables = remote(table_ref, table_ref, table_send, table_recv, {"tp": partner})
    tables.wait_recv()

    def halves():
        return [(h, jj) for jj in range(half_tiles) for h in range(2)]

    def late_pairs():
        for f in range(others):
            gathered(slot_b(f), 0, piece).wait_recv()
            for p in range(2):
                for sub in range(2):
                    pair_copy(slot_b(f), p, sub).start()

    def diagonal_pairs(sub):
        for g in range(others):
            for f in range(others):
                gathered(slot_d(g, f), sub, share).wait_recv()
                for p in range(2):
                    pair_copy(slot_d(g, f), p, sub).start()

    def batch(slot, k0, k1, send, between=None, hook=None, at=None):
        paired(slot).wait_recv()
        hidden(x_ref.at[slot], joined(k0, k1))
        if between is not None:
            between()

        def done(h, jj):
            core_ref[slot, h * half_tiles + jj] = core_sum(slot, h, jj).astype(jnp.bfloat16)
            send(h, jj)

        return partial(slot, done, LAG, hook if others == 1 else None, at)

    def batch_a(f):
        def send(h, jj):
            first_copy(h, f, 0, jj, h, slot_a(f)).start()

        def between():
            late_x(f, 1).start()
            late_y(f, 1).start()
            if others == 1:
                diagonal_pairs(0)
                weight_steps(1)

        late_x(f, 0).start()
        late_y(f, 0).start()
        ended = functools.partial(diagonal_pairs, 1)
        batch(slot_a(f), f, (f + 1) * side - 1, send, between, ended)()

    def batch_d(i):
        g, f = (i // others, i % others) if others > 1 else (0, 0)

        def send(h, jj):
            if h == 0:
                whole_copy(0, f, g + 1, jj, slot_d(g, f)).start()
            else:
                whole_copy(1, g, f + 1, jj, slot_d(g, f)).start()

        k = (g + 1) * side + f
        between = functools.partial(weight_steps, 1) if others == 1 else None
        finish = batch(slot_d(g, f), k, k, send, between, late_pairs, 1)
        if others == 1:
            return finish
        finish()

    def batch_b(f, between=None):
        def send(h, jj):
            first_copy(h, f, 0, jj, 1 - h, slot_b(f)).start()

        batch(slot_b(f), (f + 1) * side - 1, f, send, between)()

    each(others, batch_a)
    weight_steps(2)
    if others == 1:
        finish_d = batch_d(0)
        weight_steps(1)

        def between_b():
            finish_d()
            weight_steps(1)

        batch_b(0, between_b)
    else:
        diagonal_pairs(0)
        diagonal_pairs(1)
        each(others * others, batch_d)
        weight_steps(1)
        late_pairs()
        each(others, batch_b)
    weight_steps(2)

    def second_stage(g):
        for h, jj in halves():
            for late in range(2):
                p = h if late else 1 - h
                slot, j = second_slot(h, g, p), h * half_tiles + jj
                total = core_ref[slot, j, z_rows(p)].astype(jnp.float32)
                for f in range(others):
                    if not late:
                        whole_copy(h, f, g + 1, jj, slot).wait_recv()
                    total = total + first_ref[h, f, g + 1, jj, z_rows(p)].astype(jnp.float32)
                core_ref[slot, j, z_rows(p)] = total.astype(jnp.bfloat16)
                second_copy(h, g, jj, p).start()

    each(others, second_stage)

    def plane_sum(j, h, jj):
        total = acc_ref[j]
        for f in range(others):
            whole_copy(h, f, 0, jj, own).wait_recv()
            total = total + first_ref[h, f, 0, jj].astype(jnp.float32)
        for g in range(others):
            second_arrival(h, g, jj).wait_recv()
            total = total + second_ref[h, g, jj].astype(jnp.float32)
        acc_ref[j] = total

    def z_level(level, jj):
        for h in range(2):
            j = h * half_tiles + jj
            if level == 0:
                plane_sum(j, h, jj)
            else:
                z_fold(level - 1, j)
            if level < levels:
                bit, first, count = z_part(level)
                for m in range(count):
                    zsend_ref[j, first + m] = acc_ref[j, 2 * m + 1 - bit].astype(jnp.bfloat16)
                z_copy(level, j).start()

    def z_fold(level, j):
        bit, first, count = z_part(level)
        z_copy(level, j).wait_recv()
        for m in range(count):
            acc_ref[j, m] = acc_ref[j, 2 * m + bit] + zrecv_ref[j, first + m].astype(jnp.float32)

    def straight_copy(h, k):
        return remote(
            ysend_ref.at[h, z_peer(k)],
            yrecv_ref.at[h, k],
            y_send,
            y_recv,
            {"tp": z_peer(k) * 2 + core},
        )

    straight = remote(yrecv_ref, yrecv_ref, y_send, y_recv, {"tp": partner})

    def z_straight(jj):
        for h in range(2):
            plane_sum(h * half_tiles + jj, h, jj)
            ysend_ref[h] = acc_ref[h * half_tiles + jj].astype(jnp.bfloat16)
            for k in range(n_z - 1):
                straight_copy(h, k).start()

    waves = [(level, jj) for level in range(levels) for jj in range(half_tiles - 1)]
    waves.sort(key=lambda wave: (wave[1] + 2.5 * wave[0], wave[0]))
    for i, wave in enumerate(waves[:-1]):
        z_level(*wave)
        if wave == (1, 0):
            z_straight(half_tiles - 1)
        if i in (1, 2, 3):
            weight_steps(1)
    weight_steps(len(steps))
    loads[12].wait()
    weight_pairs().wait_recv()
    project(0)
    z_level(*waves[-1])
    for i in range(1, rows // PROJECT_ROWS):
        project(i)
    loads[11].wait()

    squares = 0.0
    for jj in range(half_tiles):
        if jj < half_tiles - 1:
            z_level(levels, jj)
        else:
            straight.wait_recv()
        for h in range(2):
            j = h * half_tiles + jj
            if jj < half_tiles - 1:
                total = acc_ref[j, 0]
            else:
                total = acc_ref[j, z]
                for k in range(n_z - 1):
                    total = total + yrecv_ref[h, k].astype(jnp.float32)
                acc_ref[j, 0] = total
            squares = squares + jnp.sum(total * total, axis=-1, keepdims=True)
    scale = lax.rsqrt(squares / width + EPS)
    for j in range(tiles):
        columns = slice(j * TILE, (j + 1) * TILE)
        out_ref[:, columns] = (acc_ref[j, 0] * scale * gain_ref[:, columns]).astype(jnp.bfloat16)

    half_x = x_ref.at[:, pl.ds(0, piece)]
    remote(half_x, half_x, ag_send, rim_recv, {"tp": partner}).wait_send()
    remote(half_x, half_x, pair_send, rim_recv, {"tp": partner}).wait_send()
    tables.wait_send()
    remote(first_ref, first_ref, first_send, rim_recv, {"tp": partner}).wait_send()
    remote(second_ref, second_ref, second_send, rim_recv, {"tp": partner}).wait_send()
    halved = zsend_ref.at[pl.ds(0, 2 * (half_tiles - 1))]
    remote(halved, halved, z_send, rim_recv, {"tp": partner}).wait_send()
    straight.wait_send()
    weight_pairs().wait_send()
    for where in range(n_z):
        count = (where + 1 if where + 1 < n_z else 0) + (n_z - where if where else 0)

        @pl.when(z == where)
        def _():
            weight_blocks(count).wait_send()

    rim_copy.wait_send()


def fused(operands, n_ep, n_tp):
    expert_in, routes, _, pre_gain, gate_weight, up_weight, down_weight = operands[:7]
    pool_in, pool_weight, pool_gain, out_weight = operands[8:12]
    tokens, width = expert_in.shape
    rows, channels = pool_in.shape
    experts, _, units = gate_weight.shape
    tiles, n_z, block = width // TILE, n_tp // 2, tokens // n_tp
    side = math.isqrt(n_ep)
    others, half_tiles = side - 1, tiles // 2
    dma = pltpu.SemaphoreType.DMA
    vmem = pl.BlockSpec(memory_space=pltpu.VMEM)
    hbm = pl.BlockSpec(memory_space=pltpu.HBM)
    bf16, f32 = jnp.bfloat16, jnp.float32
    buffers = [
        (routes.shape, jnp.int32),
        (routes.shape, f32),
        (pre_gain.shape, f32),
        (pre_gain.shape, f32),
        (pool_gain.shape, f32),
        (pre_gain.shape, f32),
        ((tokens, width), bf16),
        ((tokens, width), bf16),
        ((POOL_ROWS + rows, channels), bf16),
        ((rows, channels), bf16),
        (pool_weight.shape, bf16),
        ((n_tp,) + out_weight.shape, bf16),
        ((n_ep * experts, tokens), f32),
        ((n_ep - 1, n_ep * experts, tokens), f32),
        ((n_ep - 1, tokens, width), bf16),
        (gate_weight.shape, bf16),
        (up_weight.shape, bf16),
        (down_weight.shape, bf16),
        ((experts, tokens, units), bf16),
        ((tiles, n_z, 2, block, TILE), bf16),
        ((n_ep, tiles, n_z, block, TILE), bf16),
        ((2, others, side, half_tiles, n_z, block, TILE), bf16),
        ((2, others, half_tiles, n_z, block, TILE), bf16),
        ((tiles, n_z, block, TILE), f32),
        ((tiles, n_z - 1, block, TILE), bf16),
        ((tiles, n_z - 1, block, TILE), bf16),
        ((2, n_z, block, TILE), bf16),
        ((2, n_z - 1, block, TILE), bf16),
    ]
    held = sum(math.prod(shape) * jnp.dtype(kind).itemsize for shape, kind in buffers)
    return pl.pallas_call(
        functools.partial(mixer_kernel, n_ep, n_tp),
        out_shape=(pltpu.VMEM((rows, width), bf16), pltpu.VMEM((block, width), bf16)),
        in_specs=[hbm] * len(operands),
        out_specs=(vmem, vmem),
        scratch_shapes=[pltpu.VMEM(shape, kind) for shape, kind in buffers]
        + [
            dma((len(operands) + 3 * experts,)),
            dma,
            dma,
            dma,
            dma((n_ep - 1, 2)),
            dma,
            dma((n_ep - 1,)),
            dma,
            dma((2, width // WIDE)),
            dma,
            dma((2, others, side, half_tiles)),
            dma,
            dma((2, others, half_tiles)),
            dma,
            dma((n_z.bit_length() - 1, tiles)),
            dma,
            dma,
            dma,
            dma,
            dma,
            dma((2, n_z - 1, SUBS)),
            dma,
            dma,
        ],
        compiler_params=pltpu.CompilerParams(
            collective_id=0,
            has_side_effects=True,
            vmem_limit_bytes=min(67043328, held + 10 * 2**20),
        ),
        cost_estimate=pl.CostEstimate(
            flops=6 * n_ep * tokens * experts * units * width,
            bytes_accessed=64 * 2**20,
            transcendentals=0,
        ),
        name="mixer_experts",
    )(*(pltpu.with_memory_space_constraint(operand, pltpu.HBM) for operand in operands))


def out_kernel(mix_ref, out_ref, mix_hbm, out_hbm, sems):
    copies = [
        pltpu.make_async_copy(mix_ref, mix_hbm, sems.at[0]),
        pltpu.make_async_copy(out_ref, out_hbm, sems.at[1]),
    ]
    for copy in copies:
        copy.start()
    for copy in copies:
        copy.wait()


def put_out(mix, out):
    return pl.pallas_call(
        out_kernel,
        out_shape=(
            jax.ShapeDtypeStruct(mix.shape, mix.dtype),
            jax.ShapeDtypeStruct(out.shape, out.dtype),
        ),
        in_specs=[pl.BlockSpec(memory_space=pltpu.VMEM)] * 2,
        out_specs=(pl.BlockSpec(memory_space=pltpu.HBM),) * 2,
        scratch_shapes=[pltpu.SemaphoreType.DMA((2,))],
        compiler_params=pltpu.CompilerParams(vmem_limit_bytes=2**20),
        cost_estimate=pl.CostEstimate(flops=0, bytes_accessed=2 * mix.size, transcendentals=0),
        name="put_out",
    )(
        pltpu.with_memory_space_constraint(mix, pltpu.VMEM),
        pltpu.with_memory_space_constraint(out, pltpu.VMEM),
    )


def body(
    pool_in,
    pool_weight,
    pool_gain,
    out_weight,
    mix_gain,
    expert_in,
    routes,
    route_weight,
    pre_gain,
    gate_weight,
    up_weight,
    down_weight,
    post_gain,
):
    n_ep, n_tp = lax.axis_size("ep"), lax.axis_size("tp")
    operands = (
        expert_in,
        routes.T,
        route_weight.T,
        pre_gain[None, :],
        gate_weight,
        up_weight,
        down_weight,
        post_gain[None, :],
        pool_in,
        pool_weight,
        pool_gain[None, :],
        out_weight,
        mix_gain[None, :],
    )
    return put_out(*fused(operands, n_ep, n_tp))


def solution(mesh):
    return jax.shard_map(
        body,
        mesh=mesh,
        in_specs=(
            P(("ep", "tp"), None),
            P(),
            P(),
            P("tp", None),
            P(),
            P("ep", None),
            P("ep", None),
            P("ep", None),
            P(),
            P("ep", None, "tp"),
            P("ep", None, "tp"),
            P("ep", "tp", None),
            P(),
        ),
        out_specs=(P(("ep", "tp"), None), P(("ep", "tp"), None)),
        check_vma=False,
    )
```

```python
import functools
import math

import jax
import jax.numpy as jnp
from jax import lax
from jax.experimental import pallas as pl
from jax.experimental.pallas import tpu as pltpu
from jax.sharding import PartitionSpec as P

WINDOWS = (2, 4, 8, 16)
EPS = 1e-06
LIMIT = 7.0
ALPHA = 1.702
TILE = 256
WIDE = 512
LAG = 2
POOL_ROWS = 128
PROJECT_ROWS = 256
SUBS = 4
MESH = pl.DeviceIdType.MESH


def rms_scale(values, gain):
    mean_square = jnp.mean(values * values, axis=-1, keepdims=True)
    return values * lax.rsqrt(mean_square + EPS) * gain


def clamped_unit(gate, up):
    gate = jnp.minimum(gate, LIMIT)
    up = jnp.clip(up, -LIMIT, LIMIT)
    return (up + 1.0) * gate * jax.nn.sigmoid(ALPHA * gate)


def flipped(place, mask, count):
    result, bit = 0, 1
    while bit < count:
        result = result + ((place // bit + mask // bit) % 2) * bit
        bit *= 2
    return result


def each(count, step):
    if count == 1:
        step(0)
    else:
        pl.loop(0, count)(step)


def both(first, second):
    return jnp.logical_and(first, second)


def mixer_kernel(
    n_ep,
    n_tp,
    expert_hbm,
    routes_hbm,
    route_weight_hbm,
    pre_gain_hbm,
    gate_hbm,
    up_hbm,
    down_hbm,
    gain_hbm,
    pool_hbm,
    pool_weight_hbm,
    pool_gain_hbm,
    out_weight_hbm,
    mix_gain_hbm,
    mix_ref,
    out_ref,
    routes_ref,
    route_weight_ref,
    pre_gain_ref,
    gain_ref,
    pool_gain_ref,
    mix_gain_ref,
    in_ref,
    own_ref,
    padded_ref,
    mixed_ref,
    pool_weight_ref,
    all_weight_ref,
    own_table_ref,
    table_ref,
    x_ref,
    gate_ref,
    up_ref,
    down_ref,
    hid_ref,
    part_ref,
    core_ref,
    first_ref,
    send_ref,
    second_ref,
    acc_ref,
    zsend_ref,
    zrecv_ref,
    load_sem,
    table_send,
    table_recv,
    ag_send,
    ag_recv,
    pair_send,
    pair_recv,
    cs_send,
    cs_recv,
    first_send,
    first_recv,
    second_send,
    second_recv,
    z_send,
    z_recv,
    rim_send,
    rim_recv,
    w_send,
    w_recv,
    wp_send,
    wp_recv,
):
    ep, tp = lax.axis_index("ep"), lax.axis_index("tp")
    core, z = tp % 2, tp // 2
    partner = z * 2 + 1 - core
    n_z = n_tp // 2
    side = math.isqrt(n_ep)
    others = side - 1
    y, x = ep // side, ep % side
    tokens, width = in_ref.shape
    experts = gate_ref.shape[0]
    tiles = width // TILE
    half_tiles = tiles // 2
    half_z = n_z // 2
    piece = tokens // 2
    share = piece // 2
    own = n_ep - 1
    pack = WIDE // TILE
    rows = padded_ref.shape[0] - POOL_ROWS
    channels = padded_ref.shape[1]
    sub_rows = out_weight_hbm.shape[0] // SUBS

    def remote(source, target, send, recv, device):
        return pltpu.make_async_remote_copy(
            source, target, send, recv, device_id=device, device_id_type=MESH
        )

    def x_peer(f):
        return {"ep": y * side + flipped(x, f + 1, side)}

    def y_peer(f):
        return {"ep": flipped(y, f + 1, side) * side + x}

    def ep_peer(k):
        return {"ep": flipped(ep, k + 1, n_ep)}

    def z_peer(k):
        return flipped(z, k + 1, n_z)

    place = ep * n_tp + tp
    devices = n_ep * n_tp
    after, before = (place + 1) % devices, (place + devices - 1) % devices

    def at(device):
        return {"ep": device // n_tp, "tp": device % n_tp}

    barrier = pltpu.get_barrier_semaphore()
    pl.semaphore_signal(barrier, inc=1, device_id=at(after), device_id_type=MESH)
    pl.semaphore_signal(barrier, inc=1, device_id=at(before), device_id_type=MESH)
    pl.semaphore_signal(barrier, inc=1, device_id={"tp": partner}, device_id_type=MESH)
    for k in range(n_ep - 1):
        pl.semaphore_signal(barrier, inc=1, device_id=ep_peer(k), device_id_type=MESH)
    for k in range(n_z - 1):
        pl.semaphore_signal(
            barrier, inc=1, device_id={"tp": z_peer(k) * 2 + core}, device_id_type=MESH
        )

    quarters = [
        pl.ds(pl.multiple_of(p * piece + side_of * share, share), share)
        for side_of in (core, 1 - core)
        for p in range(2)
    ]
    pairs = (
        (pre_gain_hbm, pre_gain_ref),
        *((expert_hbm.at[rows_of], in_ref.at[rows_of]) for rows_of in quarters),
        (routes_hbm, routes_ref),
        (route_weight_hbm, route_weight_ref),
        (out_weight_hbm, all_weight_ref.at[tp]),
        (pool_hbm, padded_ref.at[pl.ds(POOL_ROWS, rows)]),
        (pool_weight_hbm, pool_weight_ref),
        (pool_gain_hbm, pool_gain_ref),
        (gain_hbm, gain_ref),
        (mix_gain_hbm, mix_gain_ref),
    )
    loads = [
        pltpu.make_async_copy(source, target, load_sem.at[k])
        for k, (source, target) in enumerate(pairs)
    ]

    def expert_load(e, k):
        source, target = ((gate_hbm, gate_ref), (up_hbm, up_ref), (down_hbm, down_ref))[k]
        return pltpu.make_async_copy(
            source.at[e], target.at[e], load_sem.at[len(pairs) + 3 * e + k]
        )

    for k in (0, 1, 2, 8, 3, 4, 5, 6, 7):
        loads[k].start()
    for e in range(experts):
        for k in range(2):
            expert_load(e, k).start()
    for load in loads[9:]:
        load.start()
    for e in range(experts):
        expert_load(e, 2).start()

    def norm(rows_of):
        own_ref[rows_of] = rms_scale(
            in_ref[rows_of].astype(jnp.float32), pre_gain_ref[...]
        ).astype(jnp.bfloat16)

    loads[0].wait()
    for k in range(2):
        loads[1 + k].wait()
        norm(quarters[k])
    pl.semaphore_wait(barrier, n_ep + n_z + 1)

    def slot_a(f):
        return f

    def slot_d(g, f):
        return others + g * others + f

    def slot_b(f):
        return others + others * others + f

    def turn(slot):
        return (slot + 1) % n_ep % 2

    def part_rows(p):
        return pl.ds(pl.multiple_of(p * piece + core * share, share), share)

    def half_rows(p, sub):
        size = share // 2
        return pl.ds(pl.multiple_of(p * piece + core * share + sub * size, size), size)

    def gather_copy(source, slot, p, sub, device):
        here = half_rows(p, sub)
        return remote(
            source.at[here],
            x_ref.at[slot, here],
            ag_send,
            ag_recv.at[slot, sub],
            device,
        )

    def gathered(slot, sub):
        here = x_ref.at[slot, pl.ds(0, share)]
        return remote(here, here, ag_send, ag_recv.at[slot, sub], {"tp": partner})

    def early_x(f, sub):
        return gather_copy(own_ref, slot_a(f), 0, sub, x_peer(f))

    def early_y(f, sub):
        return gather_copy(own_ref, slot_a(f), 1, sub, y_peer(f))

    def late_x(f, sub):
        return gather_copy(own_ref, slot_b(f), 1, sub, x_peer(f))

    def late_y(f, sub):
        return gather_copy(own_ref, slot_b(f), 0, sub, y_peer(f))

    def pass_y(g, f, sub):
        return gather_copy(x_ref.at[slot_a(f)], slot_d(g, f), 0, sub, y_peer(g))

    def pass_x(g, f, sub):
        return gather_copy(x_ref.at[slot_a(g)], slot_d(g, f), 1, sub, x_peer(f))

    def pair_copy(slot, p, sub):
        here = half_rows(p, sub)
        return remote(
            x_ref.at[slot, here],
            x_ref.at[slot, here],
            pair_send,
            pair_recv.at[slot],
            {"tp": partner},
        )

    def paired(slot):
        here = x_ref.at[slot, pl.ds(0, piece)]
        return remote(here, here, pair_send, pair_recv.at[slot], {"tp": partner})

    def table_copy(k):
        return remote(
            own_table_ref, table_ref.at[k], table_send, table_recv, ep_peer(k)
        )

    def core_copy(slot, j):
        return remote(
            part_ref.at[pl.ds(j, pack), :, 1 - core],
            core_ref.at[slot, pl.ds(j, pack)],
            cs_send,
            cs_recv.at[turn(slot), j // pack],
            {"tp": partner},
        )

    def core_sent(slot):
        return remote(core_ref.at[slot], core_ref.at[slot], cs_send, rim_recv, {"tp": partner})

    def z_rows(p):
        return pl.ds(p * half_z, half_z)

    def packed(jj):
        return pl.ds(jj // pack * pack, pack)

    def first_copy(h, f, jj, p, slot):
        return remote(
            core_ref.at[slot, pl.ds(h * half_tiles + jj, pack), z_rows(p)],
            first_ref.at[h, f, 0, pl.ds(jj, pack), z_rows(p)],
            first_send,
            first_recv.at[h, f, 0, jj // pack],
            x_peer(f) if h == 0 else y_peer(f),
        )

    def whole_copy(h, f, g, jj, slot):
        return remote(
            core_ref.at[slot, pl.ds(h * half_tiles + jj, pack)],
            first_ref.at[h, f, g, pl.ds(jj, pack)],
            first_send,
            first_recv.at[h, f, g, jj // pack],
            x_peer(f) if h == 0 else y_peer(f),
        )

    def first_arrival(h, f, g, jj):
        here = first_ref.at[h, f, g, packed(jj)]
        return remote(here, here, first_send, first_recv.at[h, f, g, jj // pack], {"tp": partner})

    def second_slot(h, g, p):
        return slot_a(g) if h != p else slot_b(g)

    def second_copy(h, g, jj):
        return remote(
            send_ref.at[h, g, jj],
            second_ref.at[h, g, jj],
            second_send,
            second_recv.at[h, g, jj],
            y_peer(g) if h == 0 else x_peer(g),
        )

    def second_arrival(h, g, jj):
        here = second_ref.at[h, g, jj]
        return remote(here, here, second_send, second_recv.at[h, g, jj], {"tp": partner})

    levels = n_z.bit_length() - 1

    def z_part(level):
        count = n_z >> (level + 1)
        return (z // (1 << level)) % 2, n_z - 2 * count, count

    def z_copy(level, j):
        _, first, count = z_part(level)
        return remote(
            zsend_ref.at[j, pl.ds(first, count)],
            zrecv_ref.at[j, pl.ds(first, count)],
            z_send,
            z_recv.at[level, j],
            {"tp": flipped(z, 1 << level, n_z) * 2 + core},
        )

    rim_copy = remote(
        padded_ref.at[pl.ds(POOL_ROWS + rows - 16, 16)],
        padded_ref.at[pl.ds(POOL_ROWS - 16, 16)],
        rim_send,
        rim_recv,
        at(after),
    )

    def weight_rows(block, sub):
        return all_weight_ref.at[block, pl.ds(sub * sub_rows, sub_rows)]

    def toward(d, s):
        return z - s if d == 0 else z + s

    def sends(d, s):
        if d == 0:
            return both(z + 1 < n_z, z - s >= 0)
        return both(z >= 1, z + s < n_z)

    def receives(d, s):
        return z - 1 - s >= 0 if d == 0 else z + 1 + s < n_z

    def weight_copy(d, s, sub):
        block = weight_rows(toward(d, s) * 2 + core, sub)
        target = z + 1 if d == 0 else z - 1
        return remote(
            block, block, w_send, w_recv.at[d, s, sub], {"tp": target * 2 + core}
        )

    def weight_arrival(d, s, sub):
        block = weight_rows(toward(d, s + 1) * 2 + core, sub)
        return remote(
            block, block, w_send, w_recv.at[d, s, sub], {"tp": partner}
        )

    def weight_pair(d, s, sub):
        block = weight_rows(toward(d, s + 1) * 2 + core, sub)
        return remote(block, block, wp_send, wp_recv, {"tp": partner})

    def own_pair(sub):
        block = weight_rows(tp, sub)
        return remote(block, block, wp_send, wp_recv, {"tp": partner})

    def weight_blocks(count):
        here = all_weight_ref.at[pl.ds(0, count)]
        return remote(here, here, w_send, wp_recv, {"tp": partner})

    def weight_pairs():
        here = all_weight_ref.at[pl.ds(0, n_z)]
        return remote(here, here, wp_send, wp_recv, {"tp": partner})

    def weight_step(s, sub):
        for d in range(2):

            @pl.when(receives(d, s))
            def _():
                weight_arrival(d, s, sub).wait_recv()
                weight_pair(d, s, sub).start()

            if s + 1 < n_z - 1:

                @pl.when(sends(d, s + 1))
                def _():
                    weight_copy(d, s + 1, sub).start()

    for sub in range(2):
        for f in range(others):
            early_x(f, sub).start()
            early_y(f, sub).start()
        if sub == 0:
            loads[8].wait()
            rim_copy.start()
    loads[7].wait()
    for sub in range(SUBS):
        for d in range(2):

            @pl.when(sends(d, 0))
            def _():
                weight_copy(d, 0, sub).start()

        own_pair(sub).start()
    for k in (5, 6):
        loads[k].wait()
    lanes = lax.broadcasted_iota(jnp.int32, own_table_ref.shape, 0)
    table = jnp.zeros(own_table_ref.shape, jnp.float32)
    for k in range(routes_ref.shape[0]):
        table = table + jnp.where(
            lanes == routes_ref[k : k + 1, :], route_weight_ref[k : k + 1, :], 0.0
        )
    own_table_ref[...] = table
    for k in range(n_ep - 1):
        table_copy(k).start()
    for k in range(2, 4):
        loads[1 + k].wait()
        norm(quarters[k])
    padded_ref[: POOL_ROWS - 16] = jnp.zeros((POOL_ROWS - 16, channels), jnp.bfloat16)

    def pool():
        rim_copy.wait_recv()

        @pl.when(place == 0)
        def _():
            padded_ref[POOL_ROWS - 16 : POOL_ROWS] = jnp.zeros((16, channels), jnp.bfloat16)

        for k in (9, 10):
            loads[k].wait()
        group = channels // 4
        reach = (
            lax.broadcasted_iota(jnp.int32, (POOL_ROWS, 2 * POOL_ROWS), 0)
            + POOL_ROWS
            - lax.broadcasted_iota(jnp.int32, (POOL_ROWS, 2 * POOL_ROWS), 1)
        )
        local = lax.broadcasted_iota(jnp.int32, (POOL_ROWS, 1), 0)

        @pl.loop(0, rows // POOL_ROWS)
        def _(i):
            start = pl.multiple_of(i * POOL_ROWS, POOL_ROWS)
            here = pl.ds(start, POOL_ROWS)
            there = pl.ds(start + POOL_ROWS, POOL_ROWS)
            position = place * rows + start + local
            for which, window in enumerate(WINDOWS):
                columns = slice(which * group, (which + 1) * group)
                band = jnp.where((reach >= 0) & (reach < window), 1.0, 0.0).astype(jnp.bfloat16)
                running = jnp.dot(
                    band,
                    padded_ref[pl.ds(start, 2 * POOL_ROWS), columns],
                    preferred_element_type=jnp.float32,
                )
                count = jnp.minimum(position + 1, window).astype(jnp.float32)
                diff = running / count - padded_ref[there, columns].astype(jnp.float32)
                mixed = jnp.dot(
                    diff.astype(jnp.bfloat16),
                    pool_weight_ref[which],
                    preferred_element_type=jnp.float32,
                )
                mixed_ref[here, columns] = (mixed * pool_gain_ref[:, columns]).astype(jnp.bfloat16)

    def project(i):
        here = pl.ds(i * PROJECT_ROWS, PROJECT_ROWS)
        projected = jnp.dot(
            mixed_ref[here],
            all_weight_ref[...].reshape(channels, width),
            preferred_element_type=jnp.float32,
        )
        mix_ref[here] = rms_scale(projected, mix_gain_ref[...]).astype(jnp.bfloat16)

    def hidden(values_ref, table, first=False):
        lane = lax.broadcasted_iota(jnp.int32, (tokens, table.shape[0]), 1)
        weights = jnp.transpose(table)
        for which in range(experts):
            if first:
                for k in range(2):
                    expert_load(which, k).wait()
            weight = jnp.sum(
                jnp.where(lane == ep * experts + which, weights, 0.0), axis=1, keepdims=True
            )
            values = values_ref[...]
            gate = jnp.dot(values, gate_ref[which], preferred_element_type=jnp.float32)
            up = jnp.dot(values, up_ref[which], preferred_element_type=jnp.float32)
            hid_ref[which] = (clamped_unit(gate, up) * weight).astype(jnp.bfloat16)

    last = width // WIDE

    def partial(slot, after, lag=LAG, hook=None, at=None):
        def ended(j):
            core_copy(slot, j).wait_recv()
            after(j)

        starts = [
            h * half_tiles + jj for jj in range(0, half_tiles, pack) for h in range(2)
        ]
        for i, j in enumerate(starts):
            columns = slice(j * TILE, j * TILE + WIDE)
            total = jnp.dot(
                hid_ref[0], down_ref[0, :, columns], preferred_element_type=jnp.float32
            )
            for which in range(1, experts):
                total = total + jnp.dot(
                    hid_ref[which], down_ref[which, :, columns], preferred_element_type=jnp.float32
                )
            total = total.astype(jnp.bfloat16)
            for k in range(pack):
                part_ref[j + k] = total[:, k * TILE : (k + 1) * TILE].reshape(part_ref.shape[1:])
            core_copy(slot, j).start()
            if i >= lag:
                ended(starts[i - lag])
            if hook is not None and i == (last - 1 if at is None else at):
                hook()

        def finish():
            for j in starts[len(starts) - lag :]:
                ended(j)
            core_sent(slot).wait_send()

        return finish

    def joined(k0, k1):
        return jnp.concatenate(
            [table_ref[k0, :, :piece], table_ref[k1, :, piece:]], axis=1
        )

    def core_sum(slot, j):
        return part_ref[j, :, core].astype(jnp.float32) + core_ref[slot, j].astype(jnp.float32)

    hidden(own_ref, own_table_ref[...], first=True)
    pool()
    for e in range(experts):
        expert_load(e, 2).wait()

    def own_done(j):
        for k in range(pack):
            acc_ref[j + k] = core_sum(own, j + k)

    steps = [(s, sub) for s in range(n_z - 1) for sub in range(SUBS)]

    def weight_steps(count):
        for step in steps[:count]:
            weight_step(*step)
        del steps[:count]


    def early_arrived(sub):
        for f in range(others):
            gathered(slot_a(f), sub).wait_recv()
            for g in range(others):
                pass_y(g, f, sub).start()
                pass_x(f, g, sub).start()
            for p in range(2):
                pair_copy(slot_a(f), p, sub).start()

    def early_ended():
        early_arrived(1)
        weight_steps(1)

    early_arrived(0)
    partial(own, own_done, last, early_ended)()
    tables = remote(table_ref, table_ref, table_send, table_recv, {"tp": partner})
    tables.wait_recv()

    def halves():
        return [(h, jj) for jj in range(half_tiles) for h in range(2)]

    def late_pairs(sub):
        for f in range(others):
            gathered(slot_b(f), sub).wait_recv()
            for p in range(2):
                pair_copy(slot_b(f), p, sub).start()

    def diagonal_pairs(sub):
        for g in range(others):
            for f in range(others):
                gathered(slot_d(g, f), sub).wait_recv()
                for p in range(2):
                    pair_copy(slot_d(g, f), p, sub).start()

    def batch(slot, k0, k1, send, between=None, hook=None, at=None):
        paired(slot).wait_recv()
        hidden(x_ref.at[slot], joined(k0, k1))
        if between is not None:
            between()

        def done(j):
            for k in range(pack):
                core_ref[slot, j + k] = core_sum(slot, j + k).astype(jnp.bfloat16)
            send(j // half_tiles, j % half_tiles)

        return partial(slot, done, LAG, hook if others == 1 else None, at)

    def batch_a(f):
        def send(h, jj):
            first_copy(h, f, jj, h, slot_a(f)).start()

        def between():
            late_x(f, 1).start()
            late_y(f, 1).start()
            if others == 1:
                diagonal_pairs(0)
                weight_steps(1)

        late_x(f, 0).start()
        late_y(f, 0).start()
        ended = functools.partial(diagonal_pairs, 1)
        batch(slot_a(f), f, (f + 1) * side - 1, send, between, ended)()

    def batch_d(i):
        g, f = (i // others, i % others) if others > 1 else (0, 0)

        def send(h, jj):
            if h == 0:
                whole_copy(0, f, g + 1, jj, slot_d(g, f)).start()
            else:
                whole_copy(1, g, f + 1, jj, slot_d(g, f)).start()

        k = (g + 1) * side + f

        def between():
            late_pairs(0)
            weight_steps(1)

        ended = functools.partial(late_pairs, 1)
        finish = batch(slot_d(g, f), k, k, send, between if others == 1 else None, ended)
        if others == 1:
            return finish
        finish()

    def batch_b(f, between=None):
        def send(h, jj):
            first_copy(h, f, jj, 1 - h, slot_b(f)).start()

        batch(slot_b(f), (f + 1) * side - 1, f, send, between)()

    each(others, batch_a)
    weight_steps(2)
    if others == 1:
        finish_d = batch_d(0)
        weight_steps(1)

        def between_b():
            finish_d()
            weight_steps(1)

        batch_b(0, between_b)
    else:
        diagonal_pairs(0)
        diagonal_pairs(1)
        each(others * others, batch_d)
        weight_steps(1)
        late_pairs(0)
        late_pairs(1)
        each(others, batch_b)
    weight_steps(2)

    def second_stage(g):
        for h, jj in halves():
            for f in range(others):
                if jj % pack == 0:
                    first_arrival(h, f, g + 1, jj).wait_recv()
            for p in range(2):
                total = core_ref[second_slot(h, g, p), h * half_tiles + jj, z_rows(p)].astype(
                    jnp.float32
                )
                for f in range(others):
                    total = total + first_ref[h, f, g + 1, jj, z_rows(p)].astype(jnp.float32)
                send_ref[h, g, jj, z_rows(p)] = total.astype(jnp.bfloat16)
            second_copy(h, g, jj).start()

    each(others, second_stage)

    def plane_sum(j, h, jj):
        total = acc_ref[j]
        for f in range(others):
            if jj % pack == 0:
                first_arrival(h, f, 0, jj).wait_recv()
            total = total + first_ref[h, f, 0, jj].astype(jnp.float32)
        for g in range(others):
            second_arrival(h, g, jj).wait_recv()
            total = total + second_ref[h, g, jj].astype(jnp.float32)
        acc_ref[j] = total

    def z_level(level, jj):
        for h in range(2):
            j = h * half_tiles + jj
            if level == 0:
                plane_sum(j, h, jj)
            if level > 0:
                z_fold(level - 1, j)
            if level < levels:
                bit, first, count = z_part(level)
                for m in range(count):
                    zsend_ref[j, first + m] = acc_ref[j, 2 * m + 1 - bit].astype(jnp.bfloat16)
                z_copy(level, j).start()

    def z_fold(level, j):
        bit, first, count = z_part(level)
        z_copy(level, j).wait_recv()
        for m in range(count):
            acc_ref[j, m] = acc_ref[j, 2 * m + bit] + zrecv_ref[j, first + m].astype(jnp.float32)

    waves = [(level, jj) for level in range(levels) for jj in range(half_tiles)]
    waves.sort(key=lambda wave: (wave[1] + 2.5 * wave[0], wave[0]))
    for i, wave in enumerate(waves[:-1]):
        z_level(*wave)
        if i in (1, 3):
            weight_steps(1)
        if wave == (1, 1):
            weight_steps(len(steps))
            loads[12].wait()
            weight_pairs().wait_recv()
            project(0)
    z_level(*waves[-1])
    for i in range(1, rows // PROJECT_ROWS):
        project(i)
    loads[11].wait()

    squares = 0.0
    for jj in range(half_tiles):
        z_level(levels, jj)
        for h in range(2):
            total = acc_ref[h * half_tiles + jj, 0]
            squares = squares + jnp.sum(total * total, axis=-1, keepdims=True)
    scale = lax.rsqrt(squares / width + EPS)
    for j in range(tiles):
        columns = slice(j * TILE, (j + 1) * TILE)
        out_ref[:, columns] = (acc_ref[j, 0] * scale * gain_ref[:, columns]).astype(jnp.bfloat16)

    half_x = x_ref.at[:, pl.ds(0, piece)]
    remote(half_x, half_x, ag_send, rim_recv, {"tp": partner}).wait_send()
    remote(half_x, half_x, pair_send, rim_recv, {"tp": partner}).wait_send()
    tables.wait_send()
    remote(first_ref, first_ref, first_send, rim_recv, {"tp": partner}).wait_send()
    remote(second_ref, second_ref, second_send, rim_recv, {"tp": partner}).wait_send()
    remote(zsend_ref, zsend_ref, z_send, rim_recv, {"tp": partner}).wait_send()
    weight_pairs().wait_send()
    for where in range(n_z):
        count = (where + 1 if where + 1 < n_z else 0) + (n_z - where if where else 0)

        @pl.when(z == where)
        def _():
            weight_blocks(count).wait_send()

    rim_copy.wait_send()


def fused(operands, n_ep, n_tp):
    expert_in, routes, _, pre_gain, gate_weight, up_weight, down_weight = operands[:7]
    pool_in, pool_weight, pool_gain, out_weight = operands[8:12]
    tokens, width = expert_in.shape
    rows, channels = pool_in.shape
    experts, _, units = gate_weight.shape
    tiles, n_z, block = width // TILE, n_tp // 2, tokens // n_tp
    side = math.isqrt(n_ep)
    others, half_tiles = side - 1, tiles // 2
    dma = pltpu.SemaphoreType.DMA
    vmem = pl.BlockSpec(memory_space=pltpu.VMEM)
    hbm = pl.BlockSpec(memory_space=pltpu.HBM)
    bf16, f32 = jnp.bfloat16, jnp.float32
    buffers = [
        (routes.shape, jnp.int32),
        (routes.shape, f32),
        (pre_gain.shape, f32),
        (pre_gain.shape, f32),
        (pool_gain.shape, f32),
        (pre_gain.shape, f32),
        ((tokens, width), bf16),
        ((tokens, width), bf16),
        ((POOL_ROWS + rows, channels), bf16),
        ((rows, channels), bf16),
        (pool_weight.shape, bf16),
        ((n_tp,) + out_weight.shape, bf16),
        ((n_ep * experts, tokens), f32),
        ((n_ep - 1, n_ep * experts, tokens), f32),
        ((n_ep - 1, tokens, width), bf16),
        (gate_weight.shape, bf16),
        (up_weight.shape, bf16),
        (down_weight.shape, bf16),
        ((experts, tokens, units), bf16),
        ((tiles, n_z, 2, block, TILE), bf16),
        ((n_ep, tiles, n_z, block, TILE), bf16),
        ((2, others, side, half_tiles, n_z, block, TILE), bf16),
        ((2, others, half_tiles, n_z, block, TILE), bf16),
        ((2, others, half_tiles, n_z, block, TILE), bf16),
        ((tiles, n_z, block, TILE), f32),
        ((tiles, n_z - 1, block, TILE), bf16),
        ((tiles, n_z - 1, block, TILE), bf16),
    ]
    held = sum(math.prod(shape) * jnp.dtype(kind).itemsize for shape, kind in buffers)
    return pl.pallas_call(
        functools.partial(mixer_kernel, n_ep, n_tp),
        out_shape=(pltpu.VMEM((rows, width), bf16), pltpu.VMEM((block, width), bf16)),
        in_specs=[hbm] * len(operands),
        out_specs=(vmem, vmem),
        scratch_shapes=[pltpu.VMEM(shape, kind) for shape, kind in buffers]
        + [
            dma((len(operands) + 3 * experts,)),
            dma,
            dma,
            dma,
            dma((n_ep - 1, 2)),
            dma,
            dma((n_ep - 1,)),
            dma,
            dma((2, width // WIDE)),
            dma,
            dma((2, others, side, width // WIDE // 2)),
            dma,
            dma((2, others, half_tiles)),
            dma,
            dma((n_z.bit_length() - 1, tiles)),
            dma,
            dma,
            dma,
            dma((2, n_z - 1, SUBS)),
            dma,
            dma,
        ],
        compiler_params=pltpu.CompilerParams(
            collective_id=0,
            has_side_effects=True,
            vmem_limit_bytes=min(67043328, held + 10 * 2**20),
        ),
        cost_estimate=pl.CostEstimate(
            flops=6 * n_ep * tokens * experts * units * width,
            bytes_accessed=64 * 2**20,
            transcendentals=0,
        ),
        name="mixer_experts",
    )(*(pltpu.with_memory_space_constraint(operand, pltpu.HBM) for operand in operands))


def out_kernel(mix_ref, out_ref, mix_hbm, out_hbm, sems):
    copies = [
        pltpu.make_async_copy(mix_ref, mix_hbm, sems.at[0]),
        pltpu.make_async_copy(out_ref, out_hbm, sems.at[1]),
    ]
    for copy in copies:
        copy.start()
    for copy in copies:
        copy.wait()


def put_out(mix, out):
    return pl.pallas_call(
        out_kernel,
        out_shape=(
            jax.ShapeDtypeStruct(mix.shape, mix.dtype),
            jax.ShapeDtypeStruct(out.shape, out.dtype),
        ),
        in_specs=[pl.BlockSpec(memory_space=pltpu.VMEM)] * 2,
        out_specs=(pl.BlockSpec(memory_space=pltpu.HBM),) * 2,
        scratch_shapes=[pltpu.SemaphoreType.DMA((2,))],
        compiler_params=pltpu.CompilerParams(vmem_limit_bytes=2**20),
        cost_estimate=pl.CostEstimate(flops=0, bytes_accessed=2 * mix.size, transcendentals=0),
        name="put_out",
    )(
        pltpu.with_memory_space_constraint(mix, pltpu.VMEM),
        pltpu.with_memory_space_constraint(out, pltpu.VMEM),
    )


def body(
    pool_in,
    pool_weight,
    pool_gain,
    out_weight,
    mix_gain,
    expert_in,
    routes,
    route_weight,
    pre_gain,
    gate_weight,
    up_weight,
    down_weight,
    post_gain,
):
    n_ep, n_tp = lax.axis_size("ep"), lax.axis_size("tp")
    operands = (
        expert_in,
        routes.T,
        route_weight.T,
        pre_gain[None, :],
        gate_weight,
        up_weight,
        down_weight,
        post_gain[None, :],
        pool_in,
        pool_weight,
        pool_gain[None, :],
        out_weight,
        mix_gain[None, :],
    )
    return put_out(*fused(operands, n_ep, n_tp))


def solution(mesh):
    return jax.shard_map(
        body,
        mesh=mesh,
        in_specs=(
            P(("ep", "tp"), None),
            P(),
            P(),
            P("tp", None),
            P(),
            P("ep", None),
            P("ep", None),
            P("ep", None),
            P(),
            P("ep", None, "tp"),
            P("ep", None, "tp"),
            P("ep", "tp", None),
            P(),
        ),
        out_specs=(P(("ep", "tp"), None), P(("ep", "tp"), None)),
        check_vma=False,
    )
```
